512 devices in a mesh: sp: 32 (over z, x), tp: 16 (over y, core).
Axes of the slice: x: 4, y: 8, z: 8, core: 2. Of those that a mesh axis runs over, the one named last changes fastest.
Arguments:
- ffn_input: bfloat16 [4096, 2048], P('sp', 'tp'), may hold values from -6 to 6
- out_grad: bfloat16 [4096, 2048], P('sp', 'tp'), may hold values from -6 to 6
- routes: int32 [4096, 2], P('sp'), may hold values from 0 to 31, all different within a row; in each aligned block of 128 rows (0 to 127, 128 to 255, ...) at most 10 rows name the same one
- route_weight: float32 [4096, 2], P('sp'), may hold values from 0.05 to 1
- gate_w: bfloat16 [32, 2048, 2048], P('sp', None, 'tp'), may hold values from -0.125 to 0.125
- up_w: bfloat16 [32, 2048, 2048], P('sp', None, 'tp'), may hold values from -0.125 to 0.125
- down_w: bfloat16 [32, 2048, 2048], P('sp', 'tp'), may hold values from -0.125 to 0.125
- out_proj: bfloat16 [2048, 2048], P('tp'), may hold values from -0.125 to 0.125
- rec_value: bfloat16 [4096, 2048], P('sp', 'tp'), may hold values from -6 to 6
- rate_pre: bfloat16 [4096, 2048], P('sp', 'tp'), may hold values from -6 to 6
- input_pre: bfloat16 [4096, 2048], P('sp', 'tp'), may hold values from -4 to 4
- prev_state: bfloat16 [4096, 2048], P('sp', 'tp'), may hold values from -6 to 6
- decay_param: float32 [2048], P('tp'), may hold values from 4 to 12
Outputs:
- gate_w_grad: bfloat16 [32, 2048, 2048], P('sp', None, 'tp')
- up_w_grad: bfloat16 [32, 2048, 2048], P('sp', None, 'tp')
- down_w_grad: bfloat16 [32, 2048, 2048], P('sp', 'tp')
- out_proj_grad: float32 [2048, 2048], P('sp', 'tp')
- rec_value_grad: bfloat16 [4096, 2048], P('sp', 'tp')
- rate_pre_grad: bfloat16 [4096, 2048], P('sp', 'tp')
- input_pre_grad: bfloat16 [4096, 2048], P('sp', 'tp')
The draws below stay inside these ranges and needn't reach their ends.
Inputs may be any that keep to these rules, and one draw needn't show every extreme that they name: `routes`: each token names 2 different experts. Within each aligned block of 128 tokens no expert is named more than 10 times, a bound that some block reaches.
All inputs are finite; a program needn't handle non-finite values.
Results may differ from the reference program's by a relative error of at most 0.02.
Values may be sent and summed in bfloat16 or wider, within the bound.
No kernel may reach another device: no remote copies, remote signals or barrier semaphores. Data moves between devices by JAX's collectives and lax.ppermute only.
A program may use at most 64 MiB of HBM per device.

```python
import math
import jax
import jax.numpy as jnp
import numpy as np
from jax import lax

D = 2048
DR = 2048
FF_E = 2048
TOP = 2
TOK_DEV = 128
EXPERTS = 32
TOKENS = 4096
CAP = 10
N_SP = 32
N_TP = 16


def draw_rate_pre(key, part):
    noise_key = jax.random.fold_in(key, 11)
    block_key = jax.random.fold_in(key, 12)
    blocks = (TOKENS + 127) // 128
    offsets = jax.random.uniform(block_key, (blocks, 1), jnp.float32, -2.0, 2.0)
    position_block = jnp.arange(TOKENS) // 128
    base_noise = jax.random.normal(noise_key, (TOKENS, DR), jnp.float32)
    return jnp.clip(base_noise + offsets[position_block], -6.0, 6.0).astype(jnp.bfloat16)


def draw_decay_param(key, part):
    pick_key = jax.random.fold_in(key, 21)
    fast_key = jax.random.fold_in(key, 22)
    slow_key = jax.random.fold_in(key, 23)
    fast_share = 0.5
    is_fast = jax.random.bernoulli(pick_key, fast_share, (DR,))
    fast_rate = jnp.exp(jax.random.uniform(fast_key, (DR,), jnp.float32, jnp.log(0.004), jnp.log(0.012)))
    slow_rate = jnp.exp(jax.random.uniform(slow_key, (DR,), jnp.float32, jnp.log(0.1 / TOKENS), jnp.log(0.4 / TOKENS)))
    speed_value = jnp.where(is_fast, fast_rate, slow_rate)
    return (-jnp.log(jnp.expm1(speed_value))).astype(jnp.float32)


def with_spikes(drawn, rng, source, target, parts, factor):
    def block_of(dim):
        return (jnp.arange(drawn.shape[dim]) // (drawn.shape[dim] // parts)).reshape((-1,) + (1,) * (drawn.ndim - 1 - dim))

    one_side = jax.random.permutation(rng, parts)[block_of(target)]
    far = (block_of(target) + parts // 2) % parts
    return jnp.where((block_of(source) == one_side) | (block_of(source) == far), factor * drawn, drawn)


def levels(stream_key, shape, cuts, low, high):
    def one(dim, shards_of):
        steps = jax.random.uniform(jax.random.fold_in(jax.random.fold_in(stream_key, 6), dim), (shards_of,), jnp.float32, low / len(cuts), high / len(cuts))
        return jnp.repeat(jnp.exp(steps), shape[dim] // shards_of).reshape((-1,) + (1,) * (len(shape) - dim - 1))

    level = one(*cuts[0])
    for cut in cuts[1:]:
        level = level * one(*cut)
    return level


def deal_out(stream_key, own, number, rows, number_of, top, bound, skew):
    order = jax.random.permutation(stream_key, number_of)
    heavy_load, common = portions_of(number_of, rows * top, bound, skew, True), portions_of(number_of, rows * top, bound, skew, False)
    places = jnp.arange(number_of)

    def named(sizes, offset_by):
        used = int((sizes > 0).sum())
        fixed = max(1, used // 4)
        shifted = fixed + (places - fixed + offset_by * (used - fixed)) % max(1, number_of - fixed)
        return jnp.zeros((number_of,), jnp.int32).at[order[jnp.where(places < fixed, places, shifted)]].set(jnp.asarray(sizes, jnp.int32))

    sizes = jnp.where(number % 4 == 0, named(heavy_load, number // 4), named(common, number - number // 4 - 1))
    mixed = jax.random.permutation(jax.random.fold_in(own, 3), number_of)
    source_of, receiver = mixed[0:number_of // 2 * 2:2], mixed[1:number_of // 2 * 2:2]
    slack = jnp.minimum(sizes[source_of] - 1, bound - sizes[receiver]) // 2
    slack = jnp.where((source_of == order[0]) | (receiver == order[0]) | (sizes[receiver] == 0), 0, jnp.maximum(slack, 0))
    shifted = jax.random.randint(jax.random.fold_in(own, 4), (number_of // 2,), 0, 1 << 20) % (slack + 1)
    sizes = sizes.at[source_of].add(-shifted).at[receiver].add(shifted)
    labels = jnp.searchsorted(jnp.cumsum(sizes), jnp.arange(rows * top), side="right").astype(jnp.int32)
    table = labels.reshape(top, rows).T
    table = table[jax.random.permutation(jax.random.fold_in(own, 1), rows)]
    offset_by = jax.random.randint(jax.random.fold_in(own, 2), (rows, 1), 0, top)
    return jnp.take_along_axis(table, (jnp.arange(top)[None, :] + offset_by) % top, axis=1)


def portions_of(number_of, total, bound, skew, full):
    portions = [(1 << 20) // math.isqrt(standing ** skew) + 1 for standing in range(1, number_of + 1)]
    largest = bound if full else min(bound, max(-(-total // number_of), total * portions[0] // sum(portions)))
    least = 1 if total - largest >= number_of - 1 else 0
    counts, surplus = [largest] + [least] * (number_of - 1), total - largest - least * (number_of - 1)
    while surplus > 0:
        candidates = [i for i in range(1, number_of) if counts[i] < largest] or [i for i in range(1, number_of) if counts[i] < bound]
        mass, remaining = sum([portions[i] for i in candidates]), surplus
        for i in candidates:
            more = min(bound - counts[i], max(1, remaining * portions[i] // mass), surplus)
            counts[i] = counts[i] + more
            surplus = surplus - more
    return np.array(counts)


def normal_values(key, extent, width, limit, split=(), held_as=jnp.bfloat16):
    array = jax.random.normal(key, extent, jnp.float32) * width
    if len(split) > 0:
        array = levels(key, extent, split, -0.22, 0.18) * array
    return jnp.clip(array, min=-limit, max=limit).astype(held_as)


def heavy_noise(rng, dims, scale, limit, pieces, heavy, kind=jnp.bfloat16):
    values = scale * jax.random.normal(rng, dims, jnp.float32)
    if pieces:
        values = values * levels(rng, dims, pieces, -0.22, 0.18)
    return jnp.clip(with_spikes(values, jax.random.fold_in(rng, 3), *heavy), -limit, limit).astype(kind)


def setup_inputs(seed: int = 0) -> dict:
    key_of = jax.random.split(jax.random.key(seed), 14)
    ffn_input = normal_values(key_of[0], (TOKENS, D), 1.0, 6.0, ((0, 32), (1, 16)))
    out_grad = heavy_noise(key_of[1], (TOKENS, D), 1.0, 6.0, ((0, 32), (1, 16)), (0, 1, 32, 2.75))
    routes_keys = jax.random.split(jax.random.fold_in(key_of[2], 1), TOKENS // TOK_DEV)
    routes_turns = jax.random.permutation(jax.random.fold_in(key_of[2], 3), TOKENS // TOK_DEV)
    routes = jax.vmap(lambda own, number: deal_out(jax.random.fold_in(key_of[2], 2), own, number, TOK_DEV, EXPERTS, TOP, CAP, 1))(routes_keys, routes_turns).reshape((TOKENS, TOP))
    route_weight = jnp.clip(0.05 + 0.95 * jax.random.uniform(key_of[3], (TOKENS, TOP), jnp.float32) ** levels(key_of[3], (TOKENS, TOP), ((0, 32),), -0.2, 0.2), 0.05, 1.0)
    gate_w = normal_values(key_of[4], (EXPERTS, D, FF_E), D ** -0.5, 0.125, ((0, 32), (2, 16)))
    up_w = normal_values(key_of[5], (EXPERTS, D, FF_E), D ** -0.5, 0.125, ((0, 32), (2, 16)))
    down_w = normal_values(key_of[6], (EXPERTS, FF_E, D), FF_E ** -0.5, 0.125, ((0, 32), (1, 16)))
    out_proj = normal_values(key_of[7], (DR, D), DR ** -0.5, 0.125, ((0, 16),))
    rec_value = normal_values(key_of[8], (TOKENS, DR), 1.0, 6.0, ((0, 32), (1, 16)))
    rate_pre = draw_rate_pre(jax.random.fold_in(key_of[13], 71), 0)
    input_pre = normal_values(key_of[10], (TOKENS, DR), 1.0, 4.0, ((0, 32), (1, 16)))
    prev_state = normal_values(key_of[11], (TOKENS, DR), 1.0, 6.0, ((0, 32), (1, 16)))
    decay_param = draw_decay_param(jax.random.fold_in(key_of[13], 71), 0)
    return {"ffn_input": ffn_input, "out_grad": out_grad, "routes": routes, "route_weight": route_weight, "gate_w": gate_w, "up_w": up_w, "down_w": down_w, "out_proj": out_proj, "rec_value": rec_value, "rate_pre": rate_pre, "input_pre": input_pre, "prev_state": prev_state, "decay_param": decay_param}


decay_scale = 8.0

def chain_link(left_pair, right_pair):
    return (left_pair[0] * right_pair[0], right_pair[0] * left_pair[1] + right_pair[1])

def expert_pass(rows_in, rows_cot, w_gate, w_up, w_down):
    gate_act = jnp.dot(rows_in, w_gate, preferred_element_type=jnp.float32)
    up_act = jnp.dot(rows_in, w_up, preferred_element_type=jnp.float32)
    squash = jax.nn.sigmoid(gate_act)
    silu_gate = gate_act * squash
    hidden = (silu_gate * up_act).astype(jnp.bfloat16)
    down_grad = jnp.dot(hidden.T, rows_cot, preferred_element_type=jnp.float32).astype(jnp.bfloat16)
    hidden_grad = jnp.dot(rows_cot, w_down.T, preferred_element_type=jnp.float32)
    gate_grad = (hidden_grad * up_act * squash * (1.0 + gate_act * (1.0 - squash))).astype(jnp.bfloat16)
    up_grad = (hidden_grad * silu_gate).astype(jnp.bfloat16)
    gate_w_grad = jnp.dot(rows_in.T, gate_grad, preferred_element_type=jnp.float32).astype(jnp.bfloat16)
    up_w_grad = jnp.dot(rows_in.T, up_grad, preferred_element_type=jnp.float32).astype(jnp.bfloat16)
    group_width = gate_grad.shape[1] // N_TP
    model_width = w_gate.shape[0]
    gate_parts = jnp.einsum('rjf,djf->jrd', gate_grad.reshape(-1, N_TP, group_width).astype(jnp.float32), w_gate.reshape(model_width, N_TP, group_width).astype(jnp.float32))
    up_parts = jnp.einsum('rjf,djf->jrd', up_grad.reshape(-1, N_TP, group_width).astype(jnp.float32), w_up.reshape(model_width, N_TP, group_width).astype(jnp.float32))
    group_parts = lax.optimization_barrier((gate_parts + up_parts).astype(jnp.bfloat16))
    row_grad = lax.optimization_barrier(jnp.sum(group_parts.astype(jnp.float32), axis=0)).astype(jnp.bfloat16)
    return (gate_w_grad, up_w_grad, down_grad, row_grad)

def reference(ffn_input, out_grad, routes, route_weight, gate_w, up_w, down_w, out_proj, rec_value, rate_pre, input_pre, prev_state, decay_param):
    slot_total = EXPERTS * N_SP * CAP
    flat_routes = routes.reshape(N_SP, TOK_DEV * TOP)
    route_marks = (flat_routes[:, :, None] == jnp.arange(EXPERTS, dtype=jnp.int32)[None, None, :]).astype(jnp.int32)
    before = lax.optimization_barrier(jnp.sum((jnp.cumsum(route_marks, axis=1) - route_marks) * route_marks, axis=2))
    source = jnp.arange(N_SP, dtype=jnp.int32)[:, None]
    slot_index = (flat_routes * (N_SP * CAP) + source * CAP + before).reshape(-1).astype(jnp.int32)
    route_ids = jnp.arange(TOKENS * TOP, dtype=jnp.int32)
    slot_owner = jnp.zeros((slot_total,), jnp.int32).at[slot_index].set(route_ids)
    filled = jnp.zeros((slot_total,), jnp.int32).at[slot_index].set(1)
    flat_weight = route_weight.reshape(-1)

    def one_expert(expert_items):
        w_gate, w_up, w_down, owned_route, filled_row = expert_items
        token_index = owned_route // TOP
        kept_mask = filled_row[:, None] > 0
        rows_in = jnp.where(kept_mask, ffn_input[token_index], jnp.zeros((), jnp.bfloat16))
        scaled = (flat_weight[owned_route][:, None] * out_grad[token_index].astype(jnp.float32)).astype(jnp.bfloat16)
        rows_cot = jnp.where(kept_mask, scaled, jnp.zeros((), jnp.bfloat16))
        return expert_pass(rows_in, rows_cot, w_gate, w_up, w_down)
    gate_w_grad, up_w_grad, down_w_grad, row_grad = lax.map(one_expert, (gate_w, up_w, down_w, slot_owner.reshape(EXPERTS, N_SP * CAP), filled.reshape(EXPERTS, N_SP * CAP)))
    picked = row_grad.reshape(slot_total, D)[slot_index].astype(jnp.float32).reshape(TOKENS, TOP, D)
    mix_grad = (lax.optimization_barrier(jnp.sum(picked, axis=1)) + out_grad.astype(jnp.float32)).astype(jnp.bfloat16)
    state_grad = jnp.dot(mix_grad, out_proj.T, preferred_element_type=jnp.float32)
    rate_gate = jax.nn.sigmoid(rate_pre.astype(jnp.float32))
    input_gate = jax.nn.sigmoid(input_pre.astype(jnp.float32))
    decay_speed = jax.nn.softplus(-decay_param.astype(jnp.float32))[None, :]
    log_decay = -decay_scale * rate_gate * decay_speed
    decay = jnp.exp(log_decay)
    scale_in = jnp.sqrt(-jnp.expm1(2.0 * log_decay))
    signal = rec_value.astype(jnp.float32)
    before_state = prev_state.astype(jnp.float32)
    rec_state = (decay * before_state + scale_in * input_gate * signal).astype(jnp.bfloat16)
    out_proj_grad = jnp.dot(mix_grad.T, rec_state, preferred_element_type=jnp.float32)
    following = jnp.concatenate([decay[1:], jnp.ones((1, DR), jnp.float32)], axis=0)
    _, carried = lax.associative_scan(chain_link, (following[::-1], state_grad[::-1]), axis=0)
    carried = carried[::-1]
    rec_value_grad = (carried * scale_in * input_gate).astype(jnp.bfloat16)
    input_pre_grad = (carried * scale_in * signal * input_gate * (1.0 - input_gate)).astype(jnp.bfloat16)
    decay_part = decay * before_state - input_gate * signal * decay * decay / scale_in
    rate_pre_grad = (carried * decay_part * (-decay_scale * decay_speed) * rate_gate * (1.0 - rate_gate)).astype(jnp.bfloat16)
    return (gate_w_grad, up_w_grad, down_w_grad, out_proj_grad, rec_value_grad, rate_pre_grad, input_pre_grad)
```

```python
import functools

import jax
import jax.numpy as jnp
from jax import lax
from jax.experimental import pallas as pl
from jax.experimental.pallas import tpu as pltpu
from jax.sharding import Mesh
from jax.sharding import PartitionSpec as P

SP = ("z", "x")
TP = ("y", "c")
F32 = jnp.float32
BF16 = jnp.bfloat16
decay_scale = 8.0
PAD = 16


def whole(shape, dtype):
    return jax.ShapeDtypeStruct(shape, dtype)


def dot(a, b, dims):
    return lax.dot_general(a, b, (dims, ((), ())), preferred_element_type=F32)


def expert_body(got, wg, wu, wd, gu_grad, hidden, part):
    n_c, n_y, two_rows, fw = got.shape
    rows = two_rows // 2
    hid = wg.shape[1]
    acc = jnp.zeros((rows, 2 * hid), F32)
    back = jnp.zeros((rows, hid), F32)
    for y in range(n_y):
        at = pl.ds(y * n_c * fw, n_c * fw)
        x_in = jnp.concatenate([got[c, y, :rows, :] for c in range(n_c)], axis=1)
        x_cot = jnp.concatenate([got[c, y, rows:, :] for c in range(n_c)], axis=1)
        w_both = jnp.concatenate([wg[at, :], wu[at, :]], axis=1)
        acc = acc + dot(x_in, w_both, ((1,), (0,)))
        back = back + dot(x_cot, wd[:, at], ((1,), (1,)))
    gate, up = acc[:, :hid], acc[:, hid:]
    squash = jax.nn.sigmoid(gate)
    silu = gate * squash
    hidden[...] = (silu * up).astype(BF16)
    g_grad = (back * up * squash * (1.0 + gate * (1.0 - squash))).astype(BF16)
    u_grad = (back * silu).astype(BF16)
    both = jnp.concatenate([g_grad, u_grad], axis=1)
    gu_grad[...] = both
    for y in range(n_y):
        at = pl.ds(y * n_c * fw, n_c * fw)
        w_both = jnp.concatenate([wg[at, :], wu[at, :]], axis=1)
        r = dot(both, w_both, ((1,), (1,))).astype(BF16)
        for c in range(n_c):
            part[c, y] = r[:, c * fw : (c + 1) * fw]


def expert_rows_grad(got, wg, wu, wd):
    n_c, n_y, two_rows, fw = got.shape
    rows, hid = two_rows // 2, wg.shape[1]
    return pl.pallas_call(
        expert_body,
        out_shape=(
            whole((rows, 2 * hid), BF16),
            whole((rows, hid), BF16),
            whole((n_c, n_y, rows, fw), BF16),
        ),
        name="expert_rows_grad",
    )(got, wg, wu, wd)


def weight_body(got, gu_grad, hidden, dg, du, dd):
    n_c, n_y, two_rows, fw = got.shape
    rows = two_rows // 2
    hid = hidden.shape[1]
    for y in range(n_y):
        at = pl.ds(y * n_c * fw, n_c * fw)
        x_in = jnp.concatenate([got[c, y, :rows, :] for c in range(n_c)], axis=1)
        x_cot = jnp.concatenate([got[c, y, rows:, :] for c in range(n_c)], axis=1)
        both = dot(x_in, gu_grad[...], ((0,), (0,))).astype(BF16)
        dg[at, :] = both[:, :hid]
        du[at, :] = both[:, hid:]
        dd[:, at] = dot(hidden[...], x_cot, ((0,), (0,))).astype(BF16)


def expert_weight_grads(got, gu_grad, hidden):
    n_c, n_y, _, fw = got.shape
    d, hid = n_c * n_y * fw, hidden.shape[1]
    return pl.pallas_call(
        weight_body,
        out_shape=(whole((d, hid), BF16), whole((d, hid), BF16), whole((hid, d), BF16)),
        name="expert_weight_grads",
    )(got, gu_grad, hidden)


def slot_marks(routes, experts):
    tokens, count = routes.shape
    names = routes.T
    here = [names[k][None, :] == jnp.arange(experts, dtype=jnp.int32)[:, None] for k in range(count)]
    named = functools.reduce(jnp.logical_or, here).astype(BF16)
    t = jnp.arange(tokens, dtype=jnp.int32)
    earlier = (t[:, None] < t[None, :]).astype(BF16)
    before = dot(named, earlier, ((1,), (0,)))
    row = jnp.arange(experts * PAD, dtype=jnp.int32)[:, None]
    marks = []
    for k in range(count):
        rank = jnp.sum(jnp.where(here[k], before, 0.0), axis=0).astype(jnp.int32)
        marks.append(row == (names[k] * PAD + rank)[None, :])
    return marks


def chain_link(left_pair, right_pair):
    return (left_pair[0] * right_pair[0], right_pair[0] * left_pair[1] + right_pair[1])


def in_three(v):
    hi = lax.reduce_precision(v, 8, 7)
    mid = lax.reduce_precision(v - hi, 8, 7)
    return [p.astype(BF16) for p in (hi, mid, v - hi - mid)]


def of_three(a):
    return (a[2].astype(F32) + a[1].astype(F32)) + a[0].astype(F32)


def per_device(
    ffn_input,
    out_grad,
    routes,
    route_weight,
    gate_w,
    up_w,
    down_w,
    out_proj,
    rec_value,
    rate_pre,
    input_pre,
    prev_state,
    decay_param,
):
    n_sp, n_y, n_c = lax.axis_size(SP), lax.axis_size("y"), lax.axis_size("c")
    tok, count = routes.shape
    cap = 5 * count * tok // (4 * n_sp)
    rows = n_sp * cap
    fw = ffn_input.shape[1]

    marks = slot_marks(routes, n_sp)
    pick = functools.reduce(jnp.logical_or, marks).astype(BF16)
    weight = sum(jnp.sum(jnp.where(m, route_weight.T[k][None, :], 0.0), axis=1) for k, m in enumerate(marks))
    rows_in = dot(pick, ffn_input, ((1,), (0,))).astype(BF16)
    rows_cot = (weight[:, None] * dot(pick, out_grad, ((1,), (0,)))).astype(BF16)
    send = jnp.concatenate([rows_in, rows_cot], axis=1).reshape(n_sp, PAD, 2 * fw)
    recv = lax.all_to_all(send, SP, 0, 0, tiled=True)[:, :cap]
    own = jnp.concatenate(
        [recv[:, :, :fw].reshape(rows, fw), recv[:, :, fw:].reshape(rows, fw)], axis=0
    )
    over_y = lax.all_to_all(
        jnp.broadcast_to(own[None], (n_y, 2 * rows, fw)), "y", 0, 0, tiled=True
    )
    got = lax.all_to_all(
        jnp.broadcast_to(over_y[None], (n_c, n_y, 2 * rows, fw)), "c", 0, 0, tiled=True
    )

    gu_grad, hidden, part = expert_rows_grad(got, gate_w[0], up_w[0], down_w[0])
    chip = lax.all_to_all(part, "c", 0, 0, tiled=True).astype(F32).sum(axis=0).astype(BF16)
    share = lax.all_to_all(chip, "y", 0, 0, tiled=True).astype(F32).sum(axis=0).astype(BF16)
    d_gate, d_up, d_down = expert_weight_grads(got, gu_grad, hidden)

    back = jnp.pad(share.reshape(n_sp, cap, fw), ((0, 0), (0, PAD - cap), (0, 0)))
    returned = lax.all_to_all(back, SP, 0, 0, tiled=True).reshape(n_sp * PAD, fw)
    own_grad = (dot(pick, returned, ((0,), (0,))) + out_grad.astype(F32)).astype(BF16)
    mix_grad = lax.all_gather(own_grad, TP, axis=1, tiled=True)

    rate_gate = jax.nn.sigmoid(rate_pre.astype(F32))
    input_gate = jax.nn.sigmoid(input_pre.astype(F32))
    decay_speed = jax.nn.softplus(-decay_param)[None, :]
    log_decay = -decay_scale * rate_gate * decay_speed
    decay = jnp.exp(log_decay)
    scale_in = jnp.sqrt(-jnp.expm1(2.0 * log_decay))
    signal = rec_value.astype(F32)
    before_state = prev_state.astype(F32)
    rec_state = (decay * before_state + scale_in * input_gate * signal).astype(BF16)
    following = jnp.concatenate([decay[1:], jnp.ones_like(decay[:1])], axis=0)

    state_grad = dot(mix_grad, out_proj, ((1,), (1,)))
    through, local_grad = lax.associative_scan(chain_link, (following, state_grad), axis=0, reverse=True)
    proj_part = dot(mix_grad, rec_state, ((0,), (0,))).astype(BF16)
    chain = in_three(decay[0] * through[0]) + in_three(decay[0] * local_grad[0])
    chain = jnp.pad(jnp.stack(chain), ((0, 8 - len(chain)), (0, 0)))
    width = proj_part.shape[1]
    last = jnp.concatenate(
        [
            proj_part.reshape(n_sp, -1, width),
            jnp.broadcast_to(chain[None], (n_sp, *chain.shape)),
        ],
        axis=1,
    )
    last = lax.all_to_all(last, SP, 0, 0, tiled=True)
    keep = proj_part.shape[0] // n_sp
    out_proj_grad = last[:, :keep].astype(F32).sum(axis=0)
    mult = of_three([last[:, keep + i] for i in range(3)])
    add = of_three([last[:, keep + 3 + i] for i in range(3)])
    here = lax.axis_index(SP)
    incoming = jnp.zeros_like(add[0])
    for k in reversed(range(n_sp)):
        incoming = jnp.where(k > here, add[k] + mult[k] * incoming, incoming)
    carried = local_grad + through * incoming[None, :]

    rec_value_grad = (carried * scale_in * input_gate).astype(BF16)
    input_pre_grad = (carried * scale_in * signal * input_gate * (1.0 - input_gate)).astype(BF16)
    decay_part = decay * before_state - input_gate * signal * decay * decay / scale_in
    rate_pre_grad = (
        carried * decay_part * (-decay_scale * decay_speed) * rate_gate * (1.0 - rate_gate)
    ).astype(BF16)
    return (
        d_gate[None],
        d_up[None],
        d_down[None],
        out_proj_grad,
        rec_value_grad,
        rate_pre_grad,
        input_pre_grad,
    )


def solution(mesh):
    finer = Mesh(mesh.devices.reshape(8, 4, 8, 2), ("z", "x", "y", "c"))
    grid = P(SP, TP)
    return jax.shard_map(
        per_device,
        mesh=finer,
        in_specs=(
            grid,
            grid,
            P(SP, None),
            P(SP, None),
            P(SP, None, TP),
            P(SP, None, TP),
            P(SP, TP, None),
            P(TP, None),
            grid,
            grid,
            grid,
            grid,
            P(TP),
        ),
        out_specs=(P(SP, None, TP), P(SP, None, TP), P(SP, TP, None), grid, grid, grid, grid),
        check_vma=False,
    )
```

```python
import functools

import jax
import jax.numpy as jnp
from jax import lax
from jax.experimental import pallas as pl
from jax.experimental.pallas import tpu as pltpu
from jax.sharding import Mesh
from jax.sharding import PartitionSpec as P

SP = ("z", "x")
TP = ("y", "c")
F32 = jnp.float32
BF16 = jnp.bfloat16
decay_scale = 8.0

SMEM = pl.BlockSpec(memory_space=pltpu.SMEM)
VMEM = pl.BlockSpec(memory_space=pltpu.VMEM)


def whole(shape, dtype):
    return jax.ShapeDtypeStruct(shape, dtype)


def dot(a, b, dims):
    return lax.dot_general(a, b, (dims, ((), ())), preferred_element_type=F32)


def iota(shape, dim):
    return lax.broadcasted_iota(jnp.int32, shape, dim)


def fill_body(core, routes, weights, own, peer, far, far_peer, send, pick, rows, *, experts, half):
    me = core[0]
    count, tokens = routes.shape
    slots = experts * half
    here = [iota((experts, tokens), 0) == routes[k : k + 1, :] for k in range(count)]
    named = functools.reduce(jnp.logical_or, here)
    earlier = iota((tokens, tokens), 0) < iota((tokens, tokens), 1)
    before = dot(
        jnp.where(named, 1.0, 0.0).astype(BF16), jnp.where(earlier, 1.0, 0.0).astype(BF16), ((1,), (0,))
    )
    back, mine = [], []
    for k in range(count):
        rank = jnp.sum(jnp.where(here[k], before, 0.0), axis=0, keepdims=True).astype(jnp.int32)
        name = routes[k : k + 1, :]
        back.append(name * 16 + rank + jnp.where(rank >= half, 8 - half, 0))
        at = rank - me * half
        mine.append(jnp.where((at >= 0) & (at < half), name * half + at, -1))
    hit = functools.reduce(jnp.logical_or, [iota(pick.shape, 0) == b for b in back])
    pick[...] = jnp.where(hit, 1.0, 0.0).astype(BF16)
    row = iota((slots, tokens), 0)
    hits = [row == m for m in mine]
    scale = sum(
        jnp.sum(jnp.where(h, weights[k : k + 1, :], 0.0), axis=1, keepdims=True)
        for k, h in enumerate(hits)
    )
    choose = jnp.where(functools.reduce(jnp.logical_or, hits), 1.0, 0.0).astype(BF16)
    for a in range(2):
        for n, (mine_x, peer_x) in enumerate(((own, peer), (far, far_peer))):
            for c in range(2):
                x = jnp.where(me == c, mine_x[a * tokens : (a + 1) * tokens, :], peer_x[a * tokens : (a + 1) * tokens, :])
                r = dot(choose, x, ((1,), (0,)))
                rows[pl.ds(4 * a + 2 * n + c, slots, stride=8), :] = scale * r if a else r
    send[...] = rows[...].astype(BF16)


def fill_slots(core, routes, weights, own, peer, far, far_peer, experts, half):
    fw = own.shape[1]
    total = experts * half * 8
    return pl.pallas_call(
        functools.partial(fill_body, experts=experts, half=half),
        out_shape=(whole((total, fw), BF16), whole((experts * 16, routes.shape[1]), BF16)),
        in_specs=[SMEM] + [VMEM] * 6,
        scratch_shapes=[pltpu.VMEM((total, fw), F32)],
        name="fill_slots",
    )(core, routes, weights, own, peer, far, far_peer)


def sort_body(recv, both, near, rows):
    slots = recv.shape[0] // 8
    rows[...] = recv[...].astype(F32)
    for a in range(2):
        for n in range(2):
            for c in range(2):
                v = rows[pl.ds(4 * a + 2 * n + c, slots, stride=8), :].astype(BF16)
                both[n, 2 * a + c] = v
                if n == 0:
                    near[2 * a + c] = v


def sort_pieces(recv):
    slots, fw = recv.shape[0] // 8, recv.shape[1]
    return pl.pallas_call(
        sort_body,
        out_shape=(whole((2, 4, slots, fw), BF16), whole((4, slots, fw), BF16)),
        scratch_shapes=[pltpu.VMEM(recv.shape, F32)],
        name="sort_pieces",
    )(recv)


def shards(chip, both, f1, b1, f2, b2, n_y):
    found = []
    for off, ref in ((0, both), (n_y - 1, f1), (1, b1)):
        for n in range(2):
            found.append((off + 4 * n, [ref[n, i] for i in range(4)]))
    for off, ref in ((n_y - 2, f2), (2, b2)):
        found.append((off, [ref[i] for i in range(4)]))
    for off, p in found:
        y = lax.rem(chip + off, n_y)
        yield y, jnp.concatenate(p[:2], axis=1), jnp.concatenate(p[2:], axis=1)


def expert_body(chip, both, f1, b1, f2, b2, wgu_peer, wg, wu, wd, wd_peer, gu_grad, hidden, part):
    n_y = part.shape[0]
    fw = wd.shape[0]
    rows, hid = hidden.shape
    acc = jnp.zeros((rows, 2 * hid), F32)
    back = jnp.zeros((rows, hid), F32)

    def weights(y):
        at = pl.ds(pl.multiple_of(y * 2 * fw, 2 * fw), 2 * fw)
        return jnp.concatenate([wg[at, :], wgu_peer[0, at, :], wu[at, :], wgu_peer[1, at, :]], axis=1), at

    for y, x_in, x_cot in shards(chip[0], both, f1, b1, f2, b2, n_y):
        w, at = weights(y)
        acc = acc + dot(x_in, w, ((1,), (0,)))
        back = back + dot(x_cot, jnp.concatenate([wd[:, at], wd_peer[:, at]], axis=0), ((1,), (1,)))
    gate, up = acc[:, :hid], acc[:, hid:]
    squash = jax.nn.sigmoid(gate)
    silu = gate * squash
    hidden[...] = (silu * up).astype(BF16)
    g_grad = (back * up * squash * (1.0 + gate * (1.0 - squash))).astype(BF16)
    u_grad = (back * silu).astype(BF16)
    grads = jnp.concatenate([g_grad, u_grad], axis=1)
    gu_grad[...] = grads
    for y in range(n_y):
        w, _ = weights(y)
        r = dot(grads, w, ((1,), (1,))).astype(BF16)
        part[y, 0] = r[:, :fw]
        part[y, 1] = r[:, fw:]


def expert_rows_grad(chip, blocks, wgu_peer, wg, wu, wd, wd_peer, n_y):
    rows, fw = blocks[0].shape[2:]
    hid = 2 * wg.shape[1]

    return pl.pallas_call(
        expert_body,
        out_shape=(
            whole((rows, 2 * hid), BF16),
            whole((rows, hid), BF16),
            whole((n_y, 2, rows, fw), BF16),
        ),
        in_specs=[SMEM] + [VMEM] * 10,
        name="expert_rows_grad",
    )(chip, *blocks, wgu_peer, wg, wu, wd, wd_peer)


def weight_body(chip, both, f1, b1, f2, b2, gu_grad, hidden, dgu, dgu_send, dd, dd_send):
    fw = dd.shape[0]
    hid = hidden.shape[1]
    n_y = dd.shape[1] // (2 * fw)
    for y, x_in, x_cot in shards(chip[0], both, f1, b1, f2, b2, n_y):
        at = pl.ds(pl.multiple_of(y * 2 * fw, 2 * fw), 2 * fw)
        r = dot(x_in, gu_grad[...], ((0,), (0,))).astype(BF16)
        for i in range(2):
            dgu[i, at, :] = r[:, i * hid : i * hid + fw]
            dgu_send[i, at, :] = r[:, i * hid + fw : (i + 1) * hid]
        r = dot(hidden[...], x_cot, ((0,), (0,))).astype(BF16)
        dd[:, at] = r[:fw]
        dd_send[:, at] = r[fw:]


def expert_weight_grads(chip, blocks, gu_grad, hidden, d):
    fw = blocks[0].shape[3]
    return pl.pallas_call(
        weight_body,
        out_shape=(whole((2, d, fw), BF16), whole((2, d, fw), BF16), whole((fw, d), BF16), whole((fw, d), BF16)),
        in_specs=[SMEM] + [VMEM] * 7,
        name="expert_weight_grads",
    )(chip, *blocks, gu_grad, hidden)


def add_body(parts, out, *, half):
    n_y, n_h, rows, _ = parts.shape
    j, r = iota((out.shape[0], rows), 0), iota((out.shape[0], rows), 1)
    slot = j & 7
    source = (j >> 4) * half + slot
    total = 0.0
    for h in range(n_h):
        s = parts[0, h].astype(F32)
        for y in range(1, n_y):
            s = s + parts[y, h].astype(F32)
        hit = (source == r) & (slot < half) & (((j >> 3) & 1) == h)
        total = total + dot(jnp.where(hit, 1.0, 0.0).astype(BF16), s.astype(BF16), ((1,), (0,)))
    out[...] = total.astype(BF16)


def add_parts(parts, blocks, half):
    return pl.pallas_call(
        functools.partial(add_body, half=half),
        out_shape=whole((blocks * 16, parts.shape[3]), BF16),
        name="add_parts",
    )(parts)


def chain_link(left_pair, right_pair):
    return (left_pair[0] * right_pair[0], right_pair[0] * left_pair[1] + right_pair[1])


def in_three(v):
    hi = lax.reduce_precision(v, 8, 7)
    mid = lax.reduce_precision(v - hi, 8, 7)
    return [p.astype(BF16) for p in (hi, mid, v - hi - mid)]


def of_three(a):
    return (a[2].astype(F32) + a[1].astype(F32)) + a[0].astype(F32)


def per_device(
    ffn_input,
    out_grad,
    routes,
    route_weight,
    gate_w,
    up_w,
    down_w,
    out_proj,
    rec_value,
    rate_pre,
    input_pre,
    prev_state,
    decay_param,
):
    n_sp, n_y = lax.axis_size(SP), lax.axis_size("y")
    tok, count = routes.shape
    half = 5 * count * tok // (8 * n_sp)
    fw = ffn_input.shape[1]
    d = gate_w.shape[1]
    chip = lax.axis_index("y").reshape(1).astype(jnp.int32)
    core = lax.axis_index("c").reshape(1).astype(jnp.int32)

    def over_y(v, step):
        return lax.ppermute(v, "y", [(i, (i + step) % n_y) for i in range(n_y)])

    def over_cores(v):
        return lax.ppermute(v, "c", [(0, 1), (1, 0)])

    own = jnp.concatenate([ffn_input, out_grad], axis=0)
    far = over_y(own, n_y // 2)
    far_peer = lax.ppermute(
        own, TP, [(2 * i + c, 2 * ((i + n_y // 2) % n_y) + 1 - c) for i in range(n_y) for c in range(2)]
    )
    peer = over_cores(own)
    wgu_peer = over_cores(jnp.concatenate([gate_w, up_w], axis=0))
    wd_peer = over_cores(down_w[0])

    send, pick = fill_slots(core, routes.T, route_weight.T, own, peer, far, far_peer, n_sp, half)
    recv = lax.all_to_all(send.reshape(n_sp, -1, fw), SP, 0, 0, tiled=True).reshape(send.shape)
    both, near = sort_pieces(recv)
    blocks = (both, over_y(both, 1), over_y(both, -1), over_y(near, 2), over_y(near, -2))

    gu_grad, hidden, part = expert_rows_grad(
        chip, blocks, wgu_peer, gate_w[0], up_w[0], down_w[0], wd_peer, n_y
    )
    arrived = lax.all_to_all(part.reshape(2 * n_y, *part.shape[2:]), TP, 0, 0, tiled=True)
    back = add_parts(arrived.reshape(part.shape), n_sp, half)
    returned = lax.all_to_all(back.reshape(n_sp, 16, fw), SP, 0, 0, tiled=True).reshape(back.shape)
    dgu, dgu_send, dd, dd_send = expert_weight_grads(chip, blocks, gu_grad, hidden, d)
    dgu_sum = (dgu.astype(F32) + over_cores(dgu_send).astype(F32)).astype(BF16)
    d_down = (dd.astype(F32) + over_cores(dd_send).astype(F32)).astype(BF16)
    own_grad = (dot(pick, returned, ((0,), (0,))) + out_grad.astype(F32)).astype(BF16)
    mix_grad = lax.all_gather(own_grad, TP, axis=1, tiled=True)

    rate_gate = jax.nn.sigmoid(rate_pre.astype(F32))
    input_gate = jax.nn.sigmoid(input_pre.astype(F32))
    decay_speed = jax.nn.softplus(-decay_param)[None, :]
    log_decay = -decay_scale * rate_gate * decay_speed
    decay = jnp.exp(log_decay)
    scale_in = jnp.sqrt(-jnp.expm1(2.0 * log_decay))
    signal = rec_value.astype(F32)
    before_state = prev_state.astype(F32)
    rec_state = (decay * before_state + scale_in * input_gate * signal).astype(BF16)
    following = jnp.concatenate([decay[1:], jnp.ones_like(decay[:1])], axis=0)

    state_grad = dot(mix_grad, out_proj, ((1,), (1,)))
    through, local_grad = lax.associative_scan(chain_link, (following, state_grad), axis=0, reverse=True)
    proj_part = dot(mix_grad, rec_state, ((0,), (0,))).astype(BF16)
    chain = in_three(decay[0] * through[0]) + in_three(decay[0] * local_grad[0])
    chain = jnp.pad(jnp.stack(chain), ((0, 8 - len(chain)), (0, 0)))
    width = proj_part.shape[1]
    last = jnp.concatenate(
        [
            proj_part.reshape(n_sp, -1, width),
            jnp.broadcast_to(chain[None], (n_sp, *chain.shape)),
        ],
        axis=1,
    )
    last = lax.all_to_all(last, SP, 0, 0, tiled=True)
    keep = proj_part.shape[0] // n_sp
    out_proj_grad = last[:, :keep].astype(F32).sum(axis=0)
    mult = of_three([last[:, keep + i] for i in range(3)])
    add = of_three([last[:, keep + 3 + i] for i in range(3)])
    here = lax.axis_index(SP)
    incoming = jnp.zeros_like(add[0])
    for k in reversed(range(n_sp)):
        incoming = jnp.where(k > here, add[k] + mult[k] * incoming, incoming)
    carried = local_grad + through * incoming[None, :]

    rec_value_grad = (carried * scale_in * input_gate).astype(BF16)
    input_pre_grad = (carried * scale_in * signal * input_gate * (1.0 - input_gate)).astype(BF16)
    decay_part = decay * before_state - input_gate * signal * decay * decay / scale_in
    rate_pre_grad = (
        carried * decay_part * (-decay_scale * decay_speed) * rate_gate * (1.0 - rate_gate)
    ).astype(BF16)
    return (
        dgu_sum[0][None],
        dgu_sum[1][None],
        d_down[None],
        out_proj_grad,
        rec_value_grad,
        rate_pre_grad,
        input_pre_grad,
    )


def solution(mesh):
    finer = Mesh(mesh.devices.reshape(8, 4, 8, 2), ("z", "x", "y", "c"))
    grid = P(SP, TP)
    return jax.shard_map(
        per_device,
        mesh=finer,
        in_specs=(
            grid,
            grid,
            P(SP, None),
            P(SP, None),
            P(SP, None, TP),
            P(SP, None, TP),
            P(SP, TP, None),
            P(TP, None),
            grid,
            grid,
            grid,
            grid,
            P(TP),
        ),
        out_specs=(P(SP, None, TP), P(SP, None, TP), P(SP, TP, None), grid, grid, grid, grid),
        check_vma=False,
    )
```

```python
import functools

import jax
import jax.numpy as jnp
from jax import lax
from jax.experimental import pallas as pl
from jax.experimental.pallas import tpu as pltpu
from jax.sharding import Mesh
from jax.sharding import PartitionSpec as P

SP = ("z", "x")
TP = ("y", "c")
F32 = jnp.float32
BF16 = jnp.bfloat16
decay_scale = 8.0

SMEM = pl.BlockSpec(memory_space=pltpu.SMEM)
VMEM = pl.BlockSpec(memory_space=pltpu.VMEM)


def whole(shape, dtype):
    return jax.ShapeDtypeStruct(shape, dtype)


def dot(a, b, dims):
    return lax.dot_general(a, b, (dims, ((), ())), preferred_element_type=F32)


def iota(shape, dim):
    return lax.broadcasted_iota(jnp.int32, shape, dim)


def route_body(core, routes, weights, pick, choose, scale, *, experts, half):
    me = core[0]
    count, tokens = routes.shape
    slots = experts * half
    here = [iota((experts, tokens), 0) == routes[k : k + 1, :] for k in range(count)]
    named = functools.reduce(jnp.logical_or, here)
    earlier = iota((tokens, tokens), 0) < iota((tokens, tokens), 1)
    before = dot(
        jnp.where(named, 1.0, 0.0).astype(BF16), jnp.where(earlier, 1.0, 0.0).astype(BF16), ((1,), (0,))
    )
    back, mine = [], []
    for k in range(count):
        rank = jnp.sum(jnp.where(here[k], before, 0.0), axis=0, keepdims=True).astype(jnp.int32)
        name = routes[k : k + 1, :]
        back.append(name * 16 + rank + jnp.where(rank >= half, 8 - half, 0))
        at = rank - me * half
        mine.append(jnp.where((at >= 0) & (at < half), name * half + at, -1))
    hit = functools.reduce(jnp.logical_or, [iota(pick.shape, 0) == b for b in back])
    pick[...] = jnp.where(hit, 1.0, 0.0).astype(BF16)
    row = iota((slots, tokens), 0)
    hits = [row == m for m in mine]
    scale[...] = sum(
        jnp.sum(jnp.where(h, weights[k : k + 1, :], 0.0), axis=1, keepdims=True)
        for k, h in enumerate(hits)
    )
    choose[...] = jnp.where(functools.reduce(jnp.logical_or, hits), 1.0, 0.0).astype(BF16)


def route_slots(core, routes, weights, experts, half):
    tokens, slots = routes.shape[1], experts * half
    return pl.pallas_call(
        functools.partial(route_body, experts=experts, half=half),
        out_shape=(
            whole((experts * 16, tokens), BF16),
            whole((slots, tokens), BF16),
            whole((slots, 1), F32),
        ),
        in_specs=[SMEM] + [VMEM] * 2,
        name="route_slots",
    )(core, routes, weights)


def fill_body(core, choose, scale, mine, peer, send, rows):
    me = core[0]
    slots = choose.shape[0]
    for a in range(2):
        for n in range(2):
            for c in range(2):
                x = jnp.where(me == c, mine[n, a], peer[n, a])
                r = dot(choose[...], x, ((1,), (0,)))
                rows[pl.ds(4 * a + 2 * n + c, slots, stride=8), :] = scale[...] * r if a else r
    send[...] = rows[...].astype(BF16)


def fill_slots(core, choose, scale, mine, peer):
    fw = mine.shape[-1]
    total = choose.shape[0] * 8
    return pl.pallas_call(
        fill_body,
        out_shape=whole((total, fw), BF16),
        in_specs=[SMEM] + [VMEM] * 4,
        scratch_shapes=[pltpu.VMEM((total, fw), F32)],
        name="fill_slots",
    )(core, choose, scale, mine, peer)


def sort_body(recv, both, near, rows):
    slots = recv.shape[0] // 8
    rows[...] = recv[...].astype(F32)
    for a in range(2):
        for n in range(2):
            for c in range(2):
                v = rows[pl.ds(4 * a + 2 * n + c, slots, stride=8), :].astype(BF16)
                both[n, 2 * a + c] = v
                if n == 0:
                    near[2 * a + c] = v


def sort_pieces(recv):
    slots, fw = recv.shape[0] // 8, recv.shape[1]
    return pl.pallas_call(
        sort_body,
        out_shape=(whole((2, 4, slots, fw), BF16), whole((4, slots, fw), BF16)),
        scratch_shapes=[pltpu.VMEM(recv.shape, F32)],
        name="sort_pieces",
    )(recv)


def shards(chip, both, f1, b1, f2, b2, n_y):
    found = []
    for off, ref in ((0, both), (n_y - 1, f1), (1, b1)):
        for n in range(2):
            found.append((off + 4 * n, [ref[n, i] for i in range(4)]))
    for off, ref in ((n_y - 2, f2), (2, b2)):
        found.append((off, [ref[i] for i in range(4)]))
    for off, p in found:
        y = lax.rem(chip + off, n_y)
        yield y, jnp.concatenate(p[:2], axis=1), jnp.concatenate(p[2:], axis=1)


def expert_body(chip, both, f1, b1, f2, b2, wgu_peer, wg, wu, wd, wd_peer, gu_grad, hidden, part):
    n_y = part.shape[0]
    fw = wd.shape[0]
    rows, hid = hidden.shape
    acc = jnp.zeros((rows, 2 * hid), F32)
    back = jnp.zeros((rows, hid), F32)

    def weights(y):
        at = pl.ds(pl.multiple_of(y * 2 * fw, 2 * fw), 2 * fw)
        return jnp.concatenate([wg[at, :], wgu_peer[0, at, :], wu[at, :], wgu_peer[1, at, :]], axis=1), at

    for y, x_in, x_cot in shards(chip[0], both, f1, b1, f2, b2, n_y):
        w, at = weights(y)
        acc = acc + dot(x_in, w, ((1,), (0,)))
        back = back + dot(x_cot, jnp.concatenate([wd[:, at], wd_peer[:, at]], axis=0), ((1,), (1,)))
    gate, up = acc[:, :hid], acc[:, hid:]
    squash = jax.nn.sigmoid(gate)
    silu = gate * squash
    hidden[...] = (silu * up).astype(BF16)
    g_grad = (back * up * squash * (1.0 + gate * (1.0 - squash))).astype(BF16)
    u_grad = (back * silu).astype(BF16)
    grads = jnp.concatenate([g_grad, u_grad], axis=1)
    gu_grad[...] = grads
    for y in range(n_y):
        w, _ = weights(y)
        r = dot(grads, w, ((1,), (1,))).astype(BF16)
        part[y, 0] = r[:, :fw]
        part[y, 1] = r[:, fw:]


def expert_rows_grad(chip, blocks, wgu_peer, wg, wu, wd, wd_peer, n_y):
    rows, fw = blocks[0].shape[2:]
    hid = 2 * wg.shape[1]

    return pl.pallas_call(
        expert_body,
        out_shape=(
            whole((rows, 2 * hid), BF16),
            whole((rows, hid), BF16),
            whole((n_y, 2, rows, fw), BF16),
        ),
        in_specs=[SMEM] + [VMEM] * 10,
        name="expert_rows_grad",
    )(chip, *blocks, wgu_peer, wg, wu, wd, wd_peer)


def weight_body(chip, both, f1, b1, f2, b2, gu_grad, hidden, dgu, dgu_send, dd, dd_send):
    fw = dd.shape[0]
    hid = hidden.shape[1]
    n_y = dd.shape[1] // (2 * fw)
    for y, x_in, x_cot in shards(chip[0], both, f1, b1, f2, b2, n_y):
        at = pl.ds(pl.multiple_of(y * 2 * fw, 2 * fw), 2 * fw)
        r = dot(x_in, gu_grad[...], ((0,), (0,))).astype(BF16)
        for i in range(2):
            dgu[i, at, :] = r[:, i * hid : i * hid + fw]
            dgu_send[i, at, :] = r[:, i * hid + fw : (i + 1) * hid]
        r = dot(hidden[...], x_cot, ((0,), (0,))).astype(BF16)
        dd[:, at] = r[:fw]
        dd_send[:, at] = r[fw:]


def expert_weight_grads(chip, blocks, gu_grad, hidden, d):
    fw = blocks[0].shape[3]
    return pl.pallas_call(
        weight_body,
        out_shape=(whole((2, d, fw), BF16), whole((2, d, fw), BF16), whole((fw, d), BF16), whole((fw, d), BF16)),
        in_specs=[SMEM] + [VMEM] * 7,
        name="expert_weight_grads",
    )(chip, *blocks, gu_grad, hidden)


def add_body(parts, out, *, half):
    n_y, n_h, rows, _ = parts.shape
    j, r = iota((out.shape[0], rows), 0), iota((out.shape[0], rows), 1)
    slot = j & 7
    source = (j >> 4) * half + slot
    total = 0.0
    for h in range(n_h):
        s = parts[0, h].astype(F32)
        for y in range(1, n_y):
            s = s + parts[y, h].astype(F32)
        hit = (source == r) & (slot < half) & (((j >> 3) & 1) == h)
        total = total + dot(jnp.where(hit, 1.0, 0.0).astype(BF16), s.astype(BF16), ((1,), (0,)))
    out[...] = total.astype(BF16)


def add_parts(parts, blocks, half):
    return pl.pallas_call(
        functools.partial(add_body, half=half),
        out_shape=whole((blocks * 16, parts.shape[3]), BF16),
        name="add_parts",
    )(parts)


def later(v, step, fill):
    return jnp.concatenate([v[step:], jnp.full((step, v.shape[1]), fill, v.dtype)], axis=0)


def in_three(v):
    hi = v.astype(BF16)
    mid = (v - hi.astype(F32)).astype(BF16)
    lo = (v - hi.astype(F32) - mid.astype(F32)).astype(BF16)
    return [p.astype(F32) for p in (hi, mid, lo)]


def chain_body(mix, out_proj, rec_state, decay, local, through, last):
    n_sp, width = last.shape[0], last.shape[2]
    keep = mix.shape[1] // n_sp
    proj = dot(mix[...], rec_state[...], ((0,), (0,))).astype(BF16)
    for k in range(n_sp):
        last[k, :keep, :] = proj[k * keep : (k + 1) * keep, :]
    grad = dot(mix[...], out_proj[...], ((1,), (1,)))
    mult = later(decay[...], 1, 1.0)
    step = 1
    while step < grad.shape[0]:
        grad = grad + mult * later(grad, step, 0.0)
        mult = mult * later(mult, step, 1.0)
        step *= 2
    local[...] = grad
    through[...] = mult
    first = decay[0:1, :]
    row = iota((last.shape[1] - keep, width), 0)
    chain = jnp.zeros(row.shape, F32)
    for i, piece in enumerate(in_three(first * mult[0:1, :]) + in_three(first * grad[0:1, :])):
        chain = jnp.where(row == i, piece, chain)
    chain = chain.astype(BF16)
    for k in range(n_sp):
        last[k, keep:, :] = chain


def chain_within(mix, out_proj, rec_state, decay, n_sp):
    tokens, width = decay.shape
    return pl.pallas_call(
        chain_body,
        out_shape=(
            whole((tokens, width), F32),
            whole((tokens, width), F32),
            whole((n_sp, mix.shape[1] // n_sp + 8, width), BF16),
        ),
        name="chain_within",
    )(mix, out_proj, rec_state, decay)


def finish_body(here, last, local, through, value_by, input_by, rate_by, proj, value, inp, rate):
    n_sp = last.shape[0]
    keep = proj.shape[0]
    incoming = jnp.zeros((1, last.shape[2]), F32)
    for k in reversed(range(n_sp)):
        c = last[k, keep:, :].astype(F32)
        mult = (c[2:3] + c[1:2]) + c[0:1]
        add = (c[5:6] + c[4:5]) + c[3:4]
        incoming = jnp.where(k > here[0], add + mult * incoming, incoming)
    carried = local[...] + through[...] * incoming
    value[...] = (carried * value_by[...]).astype(BF16)
    inp[...] = (carried * input_by[...]).astype(BF16)
    rate[...] = (carried * rate_by[...]).astype(BF16)
    total = last[0, :keep, :].astype(F32)
    for k in range(1, n_sp):
        total = total + last[k, :keep, :].astype(F32)
    proj[...] = total


def finish(here, last, local, through, value_by, input_by, rate_by):
    grid = whole(local.shape, BF16)
    return pl.pallas_call(
        finish_body,
        out_shape=(whole((last.shape[1] - 8, last.shape[2]), F32), grid, grid, grid),
        in_specs=[SMEM] + [VMEM] * 6,
        name="finish",
    )(here, last, local, through, value_by, input_by, rate_by)


def per_device(
    ffn_input,
    out_grad,
    routes,
    route_weight,
    gate_w,
    up_w,
    down_w,
    out_proj,
    rec_value,
    rate_pre,
    input_pre,
    prev_state,
    decay_param,
):
    n_sp, n_y = lax.axis_size(SP), lax.axis_size("y")
    tok, count = routes.shape
    half = 5 * count * tok // (8 * n_sp)
    fw = ffn_input.shape[1]
    d = gate_w.shape[1]
    chip = lax.axis_index("y").reshape(1).astype(jnp.int32)
    core = lax.axis_index("c").reshape(1).astype(jnp.int32)

    def over_y(v, step):
        return lax.ppermute(v, "y", [(i, (i + step) % n_y) for i in range(n_y)])

    def over_cores(v):
        return lax.ppermute(v, "c", [(0, 1), (1, 0)])

    own = jnp.stack([ffn_input, out_grad])
    far = over_y(own, n_y // 2)
    mine = jnp.stack([own, far])
    peer = over_cores(mine)
    pick, choose, scale = route_slots(core, routes.T, route_weight.T, n_sp, half)
    send = fill_slots(core, choose, scale, mine, peer)

    send, late_gate, late_up, late_down = lax.optimization_barrier((send, gate_w, up_w, down_w))
    wgu = jnp.concatenate([late_gate, late_up], axis=0)
    wgu_peer = over_cores(wgu)
    wd_peer = over_cores(late_down[0])
    recv = lax.all_to_all(send.reshape(n_sp, -1, fw), SP, 0, 0, tiled=True).reshape(send.shape)
    both, near = sort_pieces(recv)
    blocks = (both, over_y(both, 1), over_y(both, -1), over_y(near, 2), over_y(near, -2))

    gu_grad, hidden, part = expert_rows_grad(
        chip, blocks, wgu_peer, gate_w[0], up_w[0], down_w[0], wd_peer, n_y
    )
    arrived = lax.all_to_all(part.reshape(2 * n_y, *part.shape[2:]), TP, 0, 0, tiled=True)
    back = add_parts(arrived.reshape(part.shape), n_sp, half)
    returned = lax.all_to_all(back.reshape(n_sp, 16, fw), SP, 0, 0, tiled=True).reshape(back.shape)
    dgu, dgu_send, dd, dd_send = expert_weight_grads(chip, blocks, gu_grad, hidden, d)
    dgu_sum = (dgu.astype(F32) + over_cores(dgu_send).astype(F32)).astype(BF16)
    d_down = (dd.astype(F32) + over_cores(dd_send).astype(F32)).astype(BF16)
    own_grad = (dot(pick, returned, ((0,), (0,))) + out_grad.astype(F32)).astype(BF16)
    mix_grad = lax.all_gather(own_grad, TP, axis=1, tiled=True)

    rate_gate = jax.nn.sigmoid(rate_pre.astype(F32))
    input_gate = jax.nn.sigmoid(input_pre.astype(F32))
    decay_speed = jax.nn.softplus(-decay_param)[None, :]
    log_decay = -decay_scale * rate_gate * decay_speed
    decay = jnp.exp(log_decay)
    scale_in = jnp.sqrt(-jnp.expm1(2.0 * log_decay))
    signal = rec_value.astype(F32)
    before_state = prev_state.astype(F32)
    rec_state = (decay * before_state + scale_in * input_gate * signal).astype(BF16)
    value_by = scale_in * input_gate
    input_by = value_by * signal * (1.0 - input_gate)
    decay_part = decay * before_state - input_gate * signal * decay * decay / scale_in
    rate_by = decay_part * (-decay_scale * decay_speed) * rate_gate * (1.0 - rate_gate)

    local, through, last = chain_within(mix_grad, out_proj, rec_state, decay, n_sp)
    last = lax.all_to_all(last, SP, 0, 0, tiled=True)
    here = lax.axis_index(SP).reshape(1).astype(jnp.int32)
    out_proj_grad, rec_value_grad, input_pre_grad, rate_pre_grad = finish(
        here, last, local, through, value_by, input_by, rate_by
    )
    return (
        dgu_sum[0][None],
        dgu_sum[1][None],
        d_down[None],
        out_proj_grad,
        rec_value_grad,
        rate_pre_grad,
        input_pre_grad,
    )


def solution(mesh):
    finer = Mesh(mesh.devices.reshape(8, 4, 8, 2), ("z", "x", "y", "c"))
    grid = P(SP, TP)
    return jax.shard_map(
        per_device,
        mesh=finer,
        in_specs=(
            grid,
            grid,
            P(SP, None),
            P(SP, None),
            P(SP, None, TP),
            P(SP, None, TP),
            P(SP, TP, None),
            P(TP, None),
            grid,
            grid,
            grid,
            grid,
            P(TP),
        ),
        out_specs=(P(SP, None, TP), P(SP, None, TP), P(SP, TP, None), grid, grid, grid, grid),
        check_vma=False,
    )
```

```python
import functools

import jax
import jax.numpy as jnp
from jax import lax
from jax.experimental import pallas as pl
from jax.experimental.pallas import tpu as pltpu
from jax.sharding import Mesh
from jax.sharding import PartitionSpec as P

SP = ("z", "x")
TP = ("y", "c")
F32 = jnp.float32
BF16 = jnp.bfloat16
decay_scale = 8.0

SMEM = pl.BlockSpec(memory_space=pltpu.SMEM)
VMEM = pl.BlockSpec(memory_space=pltpu.VMEM)


def whole(shape, dtype):
    return jax.ShapeDtypeStruct(shape, dtype)


def dot(a, b, dims):
    return lax.dot_general(a, b, (dims, ((), ())), preferred_element_type=F32)


def iota(shape, dim):
    return lax.broadcasted_iota(jnp.int32, shape, dim)


def route_body(core, routes, weights, pick, choose, scale, *, experts, half):
    me = core[0]
    count, tokens = routes.shape
    slots = experts * half
    here = [iota((experts, tokens), 0) == routes[k : k + 1, :] for k in range(count)]
    named = functools.reduce(jnp.logical_or, here)
    earlier = iota((tokens, tokens), 0) < iota((tokens, tokens), 1)
    before = dot(
        jnp.where(named, 1.0, 0.0).astype(BF16), jnp.where(earlier, 1.0, 0.0).astype(BF16), ((1,), (0,))
    )
    back, mine = [], []
    for k in range(count):
        rank = jnp.sum(jnp.where(here[k], before, 0.0), axis=0, keepdims=True).astype(jnp.int32)
        name = routes[k : k + 1, :]
        back.append(name * 16 + rank + jnp.where(rank >= half, 8 - half, 0))
        at = rank - me * half
        mine.append(jnp.where((at >= 0) & (at < half), name * half + at, -1))
    hit = functools.reduce(jnp.logical_or, [iota(pick.shape, 0) == b for b in back])
    pick[...] = jnp.where(hit, 1.0, 0.0).astype(BF16)
    row = iota((slots, tokens), 0)
    hits = [row == m for m in mine]
    scale[...] = sum(
        jnp.sum(jnp.where(h, weights[k : k + 1, :], 0.0), axis=1, keepdims=True)
        for k, h in enumerate(hits)
    )
    choose[...] = jnp.where(functools.reduce(jnp.logical_or, hits), 1.0, 0.0).astype(BF16)


def route_slots(core, routes, weights, experts, half):
    tokens, slots = routes.shape[1], experts * half
    return pl.pallas_call(
        functools.partial(route_body, experts=experts, half=half),
        out_shape=(
            whole((experts * 16, tokens), BF16),
            whole((slots, tokens), BF16),
            whole((slots, 1), F32),
        ),
        in_specs=[SMEM] + [VMEM] * 2,
        name="route_slots",
    )(core, routes, weights)


def fill_body(core, choose, scale, mine, peer, send, rows):
    me = core[0]
    slots = choose.shape[0]
    for a in range(2):
        for n in range(2):
            for c in range(2):
                x = jnp.where(me == c, mine[n, a], peer[n, a])
                r = dot(choose[...], x, ((1,), (0,)))
                rows[pl.ds(4 * a + 2 * n + c, slots, stride=8), :] = scale[...] * r if a else r
    send[...] = rows[...].astype(BF16)


def fill_slots(core, choose, scale, mine, peer):
    fw = mine.shape[-1]
    total = choose.shape[0] * 8
    return pl.pallas_call(
        fill_body,
        out_shape=whole((total, fw), BF16),
        in_specs=[SMEM] + [VMEM] * 4,
        scratch_shapes=[pltpu.VMEM((total, fw), F32)],
        name="fill_slots",
    )(core, choose, scale, mine, peer)


def sort_body(recv, both, near, rows):
    slots = recv.shape[0] // 8
    rows[...] = recv[...].astype(F32)
    for a in range(2):
        for n in range(2):
            for c in range(2):
                v = rows[pl.ds(4 * a + 2 * n + c, slots, stride=8), :].astype(BF16)
                both[n, 2 * a + c] = v
                if n == 0:
                    near[2 * a + c] = v


def sort_pieces(recv):
    slots, fw = recv.shape[0] // 8, recv.shape[1]
    return pl.pallas_call(
        sort_body,
        out_shape=(whole((2, 4, slots, fw), BF16), whole((4, slots, fw), BF16)),
        scratch_shapes=[pltpu.VMEM(recv.shape, F32)],
        name="sort_pieces",
    )(recv)


def shards(chip, both, f1, b1, f2, b2, n_y):
    found = []
    for off, ref in ((0, both), (n_y - 1, f1), (1, b1)):
        for n in range(2):
            found.append((off + 4 * n, [ref[n, i] for i in range(4)]))
    for off, ref in ((n_y - 2, f2), (2, b2)):
        found.append((off, [ref[i] for i in range(4)]))
    for off, p in found:
        y = lax.rem(chip + off, n_y)
        yield y, jnp.concatenate(p[:2], axis=1), jnp.concatenate(p[2:], axis=1)


def expert_body(chip, both, f1, b1, f2, b2, wgu_peer, wg, wu, wd, wd_peer, gu_grad, hidden, part):
    n_y = part.shape[0]
    fw = wd.shape[0]
    rows, hid = hidden.shape
    acc = jnp.zeros((rows, 2 * hid), F32)
    back = jnp.zeros((rows, hid), F32)

    def weights(y):
        at = pl.ds(pl.multiple_of(y * 2 * fw, 2 * fw), 2 * fw)
        return jnp.concatenate([wg[at, :], wgu_peer[0, at, :], wu[at, :], wgu_peer[1, at, :]], axis=1), at

    for y, x_in, x_cot in shards(chip[0], both, f1, b1, f2, b2, n_y):
        w, at = weights(y)
        acc = acc + dot(x_in, w, ((1,), (0,)))
        back = back + dot(x_cot, jnp.concatenate([wd[:, at], wd_peer[:, at]], axis=0), ((1,), (1,)))
    gate, up = acc[:, :hid], acc[:, hid:]
    squash = jax.nn.sigmoid(gate)
    silu = gate * squash
    hidden[...] = (silu * up).astype(BF16)
    g_grad = (back * up * squash * (1.0 + gate * (1.0 - squash))).astype(BF16)
    u_grad = (back * silu).astype(BF16)
    grads = jnp.concatenate([g_grad, u_grad], axis=1)
    gu_grad[...] = grads
    for y in range(n_y):
        w, _ = weights(y)
        r = dot(grads, w, ((1,), (1,))).astype(BF16)
        part[y, 0] = r[:, :fw]
        part[y, 1] = r[:, fw:]


def expert_rows_grad(chip, blocks, wgu_peer, wg, wu, wd, wd_peer, n_y):
    rows, fw = blocks[0].shape[2:]
    hid = 2 * wg.shape[1]

    return pl.pallas_call(
        expert_body,
        out_shape=(
            whole((rows, 2 * hid), BF16),
            whole((rows, hid), BF16),
            whole((n_y, 2, rows, fw), BF16),
        ),
        in_specs=[SMEM] + [VMEM] * 10,
        name="expert_rows_grad",
    )(chip, *blocks, wgu_peer, wg, wu, wd, wd_peer)


def weight_body(chip, both, f1, b1, f2, b2, gu_grad, hidden, dgu, dgu_send, dd, dd_send):
    fw = dd.shape[0]
    hid = hidden.shape[1]
    n_y = dd.shape[1] // (2 * fw)
    for y, x_in, x_cot in shards(chip[0], both, f1, b1, f2, b2, n_y):
        at = pl.ds(pl.multiple_of(y * 2 * fw, 2 * fw), 2 * fw)
        r = dot(x_in, gu_grad[...], ((0,), (0,))).astype(BF16)
        for i in range(2):
            dgu[i, at, :] = r[:, i * hid : i * hid + fw]
            dgu_send[i, at, :] = r[:, i * hid + fw : (i + 1) * hid]
        r = dot(hidden[...], x_cot, ((0,), (0,))).astype(BF16)
        dd[:, at] = r[:fw]
        dd_send[:, at] = r[fw:]


def expert_weight_grads(chip, blocks, gu_grad, hidden, d):
    fw = blocks[0].shape[3]
    return pl.pallas_call(
        weight_body,
        out_shape=(whole((2, d, fw), BF16), whole((2, d, fw), BF16), whole((fw, d), BF16), whole((fw, d), BF16)),
        in_specs=[SMEM] + [VMEM] * 7,
        name="expert_weight_grads",
    )(chip, *blocks, gu_grad, hidden)


def add_body(parts, out, *, half):
    n_y, n_h, rows, _ = parts.shape
    j, r = iota((out.shape[0], rows), 0), iota((out.shape[0], rows), 1)
    slot = j & 7
    source = (j >> 4) * half + slot
    total = 0.0
    for h in range(n_h):
        s = parts[0, h].astype(F32)
        for y in range(1, n_y):
            s = s + parts[y, h].astype(F32)
        hit = (source == r) & (slot < half) & (((j >> 3) & 1) == h)
        total = total + dot(jnp.where(hit, 1.0, 0.0).astype(BF16), s.astype(BF16), ((1,), (0,)))
    out[...] = total.astype(BF16)


def add_parts(parts, blocks, half):
    return pl.pallas_call(
        functools.partial(add_body, half=half),
        out_shape=whole((blocks * 16, parts.shape[3]), BF16),
        name="add_parts",
    )(parts)


def later(v, step, fill):
    return jnp.concatenate([v[step:], jnp.full((step, v.shape[1]), fill, v.dtype)], axis=0)


def in_three(v):
    hi = v.astype(BF16)
    mid = (v - hi.astype(F32)).astype(BF16)
    lo = (v - hi.astype(F32) - mid.astype(F32)).astype(BF16)
    return [p.astype(F32) for p in (hi, mid, lo)]


def chain_body(mix, out_proj, rec_state, decay, local, through, last):
    n_sp, width = last.shape[0], last.shape[2]
    keep = mix.shape[1] // n_sp
    proj = dot(mix[...], rec_state[...], ((0,), (0,))).astype(BF16)
    for k in range(n_sp):
        last[k, :keep, :] = proj[k * keep : (k + 1) * keep, :]
    grad = dot(mix[...], out_proj[...], ((1,), (1,)))
    mult = later(decay[...], 1, 1.0)
    step = 1
    while step < grad.shape[0]:
        grad = grad + mult * later(grad, step, 0.0)
        mult = mult * later(mult, step, 1.0)
        step *= 2
    local[...] = grad
    through[...] = mult
    first = decay[0:1, :]
    row = iota((last.shape[1] - keep, width), 0)
    chain = jnp.zeros(row.shape, F32)
    for i, piece in enumerate(in_three(first * mult[0:1, :]) + in_three(first * grad[0:1, :])):
        chain = jnp.where(row == i, piece, chain)
    chain = chain.astype(BF16)
    for k in range(n_sp):
        last[k, keep:, :] = chain


def chain_within(mix, out_proj, rec_state, decay, n_sp):
    tokens, width = decay.shape
    return pl.pallas_call(
        chain_body,
        out_shape=(
            whole((tokens, width), F32),
            whole((tokens, width), F32),
            whole((n_sp, mix.shape[1] // n_sp + 8, width), BF16),
        ),
        name="chain_within",
    )(mix, out_proj, rec_state, decay)


def finish_body(here, last, local, through, value_by, input_by, rate_by, proj, value, inp, rate):
    n_sp = last.shape[0]
    keep = proj.shape[0]
    incoming = jnp.zeros((1, last.shape[2]), F32)
    for k in reversed(range(n_sp)):
        c = last[k, keep:, :].astype(F32)
        mult = (c[2:3] + c[1:2]) + c[0:1]
        add = (c[5:6] + c[4:5]) + c[3:4]
        incoming = jnp.where(k > here[0], add + mult * incoming, incoming)
    carried = local[...] + through[...] * incoming
    value[...] = (carried * value_by[...]).astype(BF16)
    inp[...] = (carried * input_by[...]).astype(BF16)
    rate[...] = (carried * rate_by[...]).astype(BF16)
    total = last[0, :keep, :].astype(F32)
    for k in range(1, n_sp):
        total = total + last[k, :keep, :].astype(F32)
    proj[...] = total


def finish(here, last, local, through, value_by, input_by, rate_by):
    grid = whole(local.shape, BF16)
    return pl.pallas_call(
        finish_body,
        out_shape=(whole((last.shape[1] - 8, last.shape[2]), F32), grid, grid, grid),
        in_specs=[SMEM] + [VMEM] * 6,
        name="finish",
    )(here, last, local, through, value_by, input_by, rate_by)


def per_device(
    ffn_input,
    out_grad,
    routes,
    route_weight,
    gate_w,
    up_w,
    down_w,
    out_proj,
    rec_value,
    rate_pre,
    input_pre,
    prev_state,
    decay_param,
):
    n_sp, n_y = lax.axis_size(SP), lax.axis_size("y")
    tok, count = routes.shape
    half = 5 * count * tok // (8 * n_sp)
    fw = ffn_input.shape[1]
    d = gate_w.shape[1]
    chip = lax.axis_index("y").reshape(1).astype(jnp.int32)
    core = lax.axis_index("c").reshape(1).astype(jnp.int32)

    def over_y(v, step):
        return lax.ppermute(v, "y", [(i, (i + step) % n_y) for i in range(n_y)])

    def over_cores(v):
        return lax.ppermute(v, "c", [(0, 1), (1, 0)])

    own = jnp.stack([ffn_input, out_grad])
    far = over_y(own, n_y // 2)
    mine = jnp.stack([own, far])
    peer = over_cores(mine)
    pick, choose, scale = route_slots(core, routes.T, route_weight.T, n_sp, half)
    send = fill_slots(core, choose, scale, mine, peer)

    send, late_gate, late_up, late_down = lax.optimization_barrier((send, gate_w, up_w, down_w))
    wgu = jnp.concatenate([late_gate, late_up], axis=0)
    wgu_peer = over_cores(wgu)
    wd_peer = over_cores(late_down[0])
    recv = lax.all_to_all(send.reshape(n_sp, -1, fw), SP, 0, 0, tiled=True).reshape(send.shape)
    both, near = sort_pieces(recv)
    blocks = (both, over_y(both, 1), over_y(both, -1), over_y(near, 2), over_y(near, -2))

    gu_grad, hidden, part = expert_rows_grad(
        chip, blocks, wgu_peer, gate_w[0], up_w[0], down_w[0], wd_peer, n_y
    )
    arrived = lax.all_to_all(part.reshape(2 * n_y, *part.shape[2:]), TP, 0, 0, tiled=True)
    back = add_parts(arrived.reshape(part.shape), n_sp, half)
    returned = lax.all_to_all(back.reshape(n_sp, 16, fw), SP, 0, 0, tiled=True).reshape(back.shape)
    dgu, dgu_send, dd, dd_send = expert_weight_grads(chip, blocks, gu_grad, hidden, d)
    dgu_peer = over_cores(dgu_send)
    dd_peer = over_cores(dd_send)
    dgu_sum = (dgu.astype(F32) + dgu_peer.astype(F32)).astype(BF16)
    d_down = (dd.astype(F32) + dd_peer.astype(F32)).astype(BF16)
    own_grad = (dot(pick, returned, ((0,), (0,))) + out_grad.astype(F32)).astype(BF16)
    mix_grad = lax.all_gather(own_grad, TP, axis=1, tiled=True)

    rate_gate = jax.nn.sigmoid(rate_pre.astype(F32))
    input_gate = jax.nn.sigmoid(input_pre.astype(F32))
    decay_speed = jax.nn.softplus(-decay_param)[None, :]
    log_decay = -decay_scale * rate_gate * decay_speed
    decay = jnp.exp(log_decay)
    scale_in = jnp.sqrt(-jnp.expm1(2.0 * log_decay))
    signal = rec_value.astype(F32)
    before_state = prev_state.astype(F32)
    rec_state = (decay * before_state + scale_in * input_gate * signal).astype(BF16)
    value_by = scale_in * input_gate
    input_by = value_by * signal * (1.0 - input_gate)
    decay_part = decay * before_state - input_gate * signal * decay * decay / scale_in
    rate_by = decay_part * (-decay_scale * decay_speed) * rate_gate * (1.0 - rate_gate)

    local, through, last = chain_within(mix_grad, out_proj, rec_state, decay, n_sp)
    last = lax.all_to_all(last, SP, 0, 0, tiled=True)
    here = lax.axis_index(SP).reshape(1).astype(jnp.int32)
    out_proj_grad, rec_value_grad, input_pre_grad, rate_pre_grad = finish(
        here, last, local, through, value_by, input_by, rate_by
    )
    return (
        dgu_sum[0][None],
        dgu_sum[1][None],
        d_down[None],
        out_proj_grad,
        rec_value_grad,
        rate_pre_grad,
        input_pre_grad,
    )


def solution(mesh):
    finer = Mesh(mesh.devices.reshape(8, 4, 8, 2), ("z", "x", "y", "c"))
    grid = P(SP, TP)
    return jax.shard_map(
        per_device,
        mesh=finer,
        in_specs=(
            grid,
            grid,
            P(SP, None),
            P(SP, None),
            P(SP, None, TP),
            P(SP, None, TP),
            P(SP, TP, None),
            P(TP, None),
            grid,
            grid,
            grid,
            grid,
            P(TP),
        ),
        out_specs=(P(SP, None, TP), P(SP, None, TP), P(SP, TP, None), grid, grid, grid, grid),
        check_vma=False,
    )
```

```python
import functools

import jax
import jax.numpy as jnp
from jax import lax
from jax.experimental import pallas as pl
from jax.experimental.pallas import tpu as pltpu
from jax.sharding import Mesh
from jax.sharding import PartitionSpec as P

SP = ("z", "x")
TP = ("y", "c")
F32 = jnp.float32
BF16 = jnp.bfloat16
decay_scale = 8.0

SMEM = pl.BlockSpec(memory_space=pltpu.SMEM)
VMEM = pl.BlockSpec(memory_space=pltpu.VMEM)


def whole(shape, dtype):
    return jax.ShapeDtypeStruct(shape, dtype)


def call(body, out, *operands, scalars=0, scratch=(), loose=(), kept=()):
    held = [
        o if i < scalars or i in loose else pltpu.with_memory_space_constraint(o, pltpu.VMEM)
        for i, o in enumerate(operands)
    ]
    outs = [(pltpu.VMEM if i in kept else pltpu.HBM)(o.shape, o.dtype) for i, o in enumerate(out)]
    got = pl.pallas_call(
        body,
        out_shape=tuple(outs),
        in_specs=[SMEM] * scalars + [VMEM] * (len(operands) - scalars),
        out_specs=tuple([VMEM] * len(outs)),
        scratch_shapes=list(scratch),
        compiler_params=pltpu.CompilerParams(vmem_limit_bytes=16 * 2**20),
    )(*held)
    return got if len(out) > 1 else got[0]


def dot(a, b, dims):
    return lax.dot_general(a, b, (dims, ((), ())), preferred_element_type=F32)


def iota(shape, dim):
    return lax.broadcasted_iota(jnp.int32, shape, dim)


def route_body(core, routes, weights, pick, choose, scale, *, experts, half):
    me = core[0]
    count, tokens = routes.shape
    slots = experts * half
    here = [iota((experts, tokens), 0) == routes[k : k + 1, :] for k in range(count)]
    named = functools.reduce(jnp.logical_or, here)
    earlier = iota((tokens, tokens), 0) < iota((tokens, tokens), 1)
    before = dot(
        jnp.where(named, 1.0, 0.0).astype(BF16), jnp.where(earlier, 1.0, 0.0).astype(BF16), ((1,), (0,))
    )
    back, mine = [], []
    for k in range(count):
        rank = jnp.sum(jnp.where(here[k], before, 0.0), axis=0, keepdims=True).astype(jnp.int32)
        name = routes[k : k + 1, :]
        back.append(name * 16 + rank + jnp.where(rank >= half, 8 - half, 0))
        at = rank - me * half
        mine.append(jnp.where((at >= 0) & (at < half), name * half + at, -1))
    hit = functools.reduce(jnp.logical_or, [iota(pick.shape, 0) == b for b in back])
    pick[...] = jnp.where(hit, 1.0, 0.0).astype(BF16)
    row = iota((slots, tokens), 0)
    hits = [row == m for m in mine]
    scale[...] = sum(
        jnp.sum(jnp.where(h, weights[k : k + 1, :], 0.0), axis=1, keepdims=True)
        for k, h in enumerate(hits)
    )
    choose[...] = jnp.where(functools.reduce(jnp.logical_or, hits), 1.0, 0.0).astype(BF16)


def route_slots(core, routes, weights, experts, half):
    tokens, slots = routes.shape[1], experts * half
    out = (whole((experts * 16, tokens), BF16), whole((slots, tokens), BF16), whole((slots, 1), F32))
    body = functools.partial(route_body, experts=experts, half=half)
    return call(body, out, core, routes, weights, scalars=1, loose=(1, 2), kept=(1, 2))


def fill_body(core, choose, scale, mine, peer, send, rows):
    me = core[0]
    slots = choose.shape[0]
    for a in range(2):
        for n in range(2):
            for c in range(2):
                x = jnp.where(me == c, mine[n, a], peer[n, a])
                r = dot(choose[...], x, ((1,), (0,)))
                rows[pl.ds(4 * a + 2 * n + c, slots, stride=8), :] = scale[...] * r if a else r
    send[...] = rows[...].astype(BF16)


def fill_slots(core, choose, scale, mine, peer):
    fw = mine.shape[-1]
    total = choose.shape[0] * 8
    out = (whole((total, fw), BF16),)
    scratch = [pltpu.VMEM((total, fw), F32)]
    return call(fill_body, out, core, choose, scale, mine, peer, scalars=1, scratch=scratch)


def sort_body(recv, both, near, rows):
    slots = recv.shape[0] // 8
    rows[...] = recv[...].astype(F32)
    for a in range(2):
        for n in range(2):
            for c in range(2):
                v = rows[pl.ds(4 * a + 2 * n + c, slots, stride=8), :].astype(BF16)
                both[n, 2 * a + c] = v
                if n == 0:
                    near[2 * a + c] = v


def sort_pieces(recv):
    slots, fw = recv.shape[0] // 8, recv.shape[1]
    out = (whole((2, 4, slots, fw), BF16), whole((4, slots, fw), BF16))
    return call(sort_body, out, recv, scratch=[pltpu.VMEM(recv.shape, F32)], kept=(0, 1))


def shards(chip, both, f1, b1, f2, b2, n_y):
    found = []
    for off, ref in ((0, both), (n_y - 1, f1), (1, b1)):
        for n in range(2):
            found.append((off + 4 * n, [ref[n, i] for i in range(4)]))
    for off, ref in ((n_y - 2, f2), (2, b2)):
        found.append((off, [ref[i] for i in range(4)]))
    for off, p in found:
        y = lax.rem(chip + off, n_y)
        yield y, jnp.concatenate(p[:2], axis=1), jnp.concatenate(p[2:], axis=1)


def expert_body(chip, both, f1, b1, f2, b2, wgu_peer, wg, wu, wd, wd_peer, gu_grad, hidden, part):
    n_y = part.shape[0]
    fw = wd.shape[0]
    rows, hid = hidden.shape
    acc = jnp.zeros((rows, 2 * hid), F32)
    back = jnp.zeros((rows, hid), F32)

    def weights(y):
        at = pl.ds(pl.multiple_of(y * 2 * fw, 2 * fw), 2 * fw)
        return jnp.concatenate([wg[at, :], wgu_peer[0, at, :], wu[at, :], wgu_peer[1, at, :]], axis=1), at

    for y, x_in, x_cot in shards(chip[0], both, f1, b1, f2, b2, n_y):
        w, at = weights(y)
        acc = acc + dot(x_in, w, ((1,), (0,)))
        back = back + dot(x_cot, jnp.concatenate([wd[:, at], wd_peer[:, at]], axis=0), ((1,), (1,)))
    gate, up = acc[:, :hid], acc[:, hid:]
    squash = jax.nn.sigmoid(gate)
    silu = gate * squash
    hidden[...] = (silu * up).astype(BF16)
    g_grad = (back * up * squash * (1.0 + gate * (1.0 - squash))).astype(BF16)
    u_grad = (back * silu).astype(BF16)
    grads = jnp.concatenate([g_grad, u_grad], axis=1)
    gu_grad[...] = grads
    for y in range(n_y):
        w, _ = weights(y)
        r = dot(grads, w, ((1,), (1,))).astype(BF16)
        part[y, 0] = r[:, :fw]
        part[y, 1] = r[:, fw:]


def expert_rows_grad(chip, blocks, wgu_peer, wg, wu, wd, wd_peer, n_y):
    rows, fw = blocks[0].shape[2:]
    hid = 2 * wg.shape[1]

    out = (whole((rows, 2 * hid), BF16), whole((rows, hid), BF16), whole((n_y, 2, rows, fw), BF16))
    weights = (wgu_peer, wg, wu, wd, wd_peer)
    return call(expert_body, out, chip, *blocks, *weights, scalars=1)


def weight_body(chip, both, f1, b1, f2, b2, gu_grad, hidden, dgu, dgu_send, dd, dd_send):
    fw = dd.shape[0]
    hid = hidden.shape[1]
    n_y = dd.shape[1] // (2 * fw)
    for y, x_in, x_cot in shards(chip[0], both, f1, b1, f2, b2, n_y):
        at = pl.ds(pl.multiple_of(y * 2 * fw, 2 * fw), 2 * fw)
        r = dot(x_in, gu_grad[...], ((0,), (0,))).astype(BF16)
        for i in range(2):
            dgu[i, at, :] = r[:, i * hid : i * hid + fw]
            dgu_send[i, at, :] = r[:, i * hid + fw : (i + 1) * hid]
        r = dot(hidden[...], x_cot, ((0,), (0,))).astype(BF16)
        dd[:, at] = r[:fw]
        dd_send[:, at] = r[fw:]


def expert_weight_grads(chip, blocks, gu_grad, hidden, d):
    fw = blocks[0].shape[3]
    out = (whole((2, d, fw), BF16),) * 2 + (whole((fw, d), BF16),) * 2
    return call(weight_body, out, chip, *blocks, gu_grad, hidden, scalars=1, loose=(6, 7))


def add_body(parts, out, *, half):
    n_y, n_h, rows, _ = parts.shape
    j, r = iota((out.shape[0], rows), 0), iota((out.shape[0], rows), 1)
    slot = j & 7
    source = (j >> 4) * half + slot
    total = 0.0
    for h in range(n_h):
        s = parts[0, h].astype(F32)
        for y in range(1, n_y):
            s = s + parts[y, h].astype(F32)
        hit = (source == r) & (slot < half) & (((j >> 3) & 1) == h)
        total = total + dot(jnp.where(hit, 1.0, 0.0).astype(BF16), s.astype(BF16), ((1,), (0,)))
    out[...] = total.astype(BF16)


def add_parts(parts, blocks, half):
    out = (whole((blocks * 16, parts.shape[3]), BF16),)
    return call(functools.partial(add_body, half=half), out, parts)


def later(v, step, fill):
    return jnp.concatenate([v[step:], jnp.full((step, v.shape[1]), fill, v.dtype)], axis=0)


def in_three(v):
    hi = v.astype(BF16)
    mid = (v - hi.astype(F32)).astype(BF16)
    lo = (v - hi.astype(F32) - mid.astype(F32)).astype(BF16)
    return [p.astype(F32) for p in (hi, mid, lo)]


def chain_body(mix, out_proj, rec_state, decay, local, through, last):
    n_sp, width = last.shape[0], last.shape[2]
    keep = mix.shape[1] // n_sp
    proj = dot(mix[...], rec_state[...], ((0,), (0,))).astype(BF16)
    for k in range(n_sp):
        last[k, :keep, :] = proj[k * keep : (k + 1) * keep, :]
    grad = dot(mix[...], out_proj[...], ((1,), (1,)))
    mult = later(decay[...], 1, 1.0)
    step = 1
    while step < grad.shape[0]:
        grad = grad + mult * later(grad, step, 0.0)
        mult = mult * later(mult, step, 1.0)
        step *= 2
    local[...] = grad
    through[...] = mult
    first = decay[0:1, :]
    row = iota((last.shape[1] - keep, width), 0)
    chain = jnp.zeros(row.shape, F32)
    for i, piece in enumerate(in_three(first * mult[0:1, :]) + in_three(first * grad[0:1, :])):
        chain = jnp.where(row == i, piece, chain)
    chain = chain.astype(BF16)
    for k in range(n_sp):
        last[k, keep:, :] = chain


def chain_within(mix, out_proj, rec_state, decay, n_sp):
    tokens, width = decay.shape
    last = whole((n_sp, mix.shape[1] // n_sp + 8, width), BF16)
    out = (whole((tokens, width), F32),) * 2 + (last,)
    return call(chain_body, out, mix, out_proj, rec_state, decay, kept=(0, 1))


def finish_body(here, last, local, through, value_by, input_by, rate_by, proj, value, inp, rate):
    n_sp = last.shape[0]
    keep = proj.shape[0]
    incoming = jnp.zeros((1, last.shape[2]), F32)
    for k in reversed(range(n_sp)):
        c = last[k, keep:, :].astype(F32)
        mult = (c[2:3] + c[1:2]) + c[0:1]
        add = (c[5:6] + c[4:5]) + c[3:4]
        incoming = jnp.where(k > here[0], add + mult * incoming, incoming)
    carried = local[...] + through[...] * incoming
    value[...] = (carried * value_by[...]).astype(BF16)
    inp[...] = (carried * input_by[...]).astype(BF16)
    rate[...] = (carried * rate_by[...]).astype(BF16)
    total = last[0, :keep, :].astype(F32)
    for k in range(1, n_sp):
        total = total + last[k, :keep, :].astype(F32)
    proj[...] = total


def finish(here, last, local, through, value_by, input_by, rate_by):
    grid = whole(local.shape, BF16)
    out = (whole((last.shape[1] - 8, last.shape[2]), F32), grid, grid, grid)
    return call(finish_body, out, here, last, local, through, value_by, input_by, rate_by, scalars=1)


def per_device(
    ffn_input,
    out_grad,
    routes,
    route_weight,
    gate_w,
    up_w,
    down_w,
    out_proj,
    rec_value,
    rate_pre,
    input_pre,
    prev_state,
    decay_param,
):
    n_sp, n_y = lax.axis_size(SP), lax.axis_size("y")
    tok, count = routes.shape
    half = 5 * count * tok // (8 * n_sp)
    fw = ffn_input.shape[1]
    d = gate_w.shape[1]
    chip = lax.axis_index("y").reshape(1).astype(jnp.int32)
    core = lax.axis_index("c").reshape(1).astype(jnp.int32)

    def over_y(v, step):
        return lax.ppermute(v, "y", [(i, (i + step) % n_y) for i in range(n_y)])

    def over_cores(v):
        return lax.ppermute(v, "c", [(0, 1), (1, 0)])

    own = jnp.stack([ffn_input, out_grad])
    far = over_y(own, n_y // 2)
    mine = jnp.stack([own, far])
    peer = over_cores(mine)
    pick, choose, scale = route_slots(core, routes.T, route_weight.T, n_sp, half)
    send = fill_slots(core, choose, scale, mine, peer)

    send, late_gate, late_up, late_down = lax.optimization_barrier((send, gate_w, up_w, down_w))
    wgu = jnp.concatenate([late_gate, late_up], axis=0)
    wgu_peer = over_cores(wgu)
    wd_peer = over_cores(late_down[0])
    recv = lax.all_to_all(send.reshape(n_sp, -1, fw), SP, 0, 0, tiled=True).reshape(send.shape)
    both, near = sort_pieces(recv)
    blocks = (both, over_y(both, 1), over_y(both, -1), over_y(near, 2), over_y(near, -2))

    gu_grad, hidden, part = expert_rows_grad(
        chip, blocks, wgu_peer, late_gate[0], late_up[0], late_down[0], wd_peer, n_y
    )
    arrived = lax.all_to_all(part.reshape(2 * n_y, *part.shape[2:]), TP, 0, 0, tiled=True)
    back = add_parts(arrived.reshape(part.shape), n_sp, half)
    returned = lax.all_to_all(back.reshape(n_sp, 16, fw), SP, 0, 0, tiled=True).reshape(back.shape)
    dgu, dgu_send, dd, dd_send = expert_weight_grads(chip, blocks, gu_grad, hidden, d)
    dgu_peer = over_cores(dgu_send)
    dd_peer = over_cores(dd_send)
    dgu_sum = (dgu.astype(F32) + dgu_peer.astype(F32)).astype(BF16)
    d_down = (dd.astype(F32) + dd_peer.astype(F32)).astype(BF16)
    own_grad = (dot(pick, returned, ((0,), (0,))) + out_grad.astype(F32)).astype(BF16)
    mix_grad = lax.all_gather(own_grad, TP, axis=1, tiled=True)

    rate_gate = jax.nn.sigmoid(rate_pre.astype(F32))
    input_gate = jax.nn.sigmoid(input_pre.astype(F32))
    decay_speed = jax.nn.softplus(-decay_param)[None, :]
    log_decay = -decay_scale * rate_gate * decay_speed
    decay = jnp.exp(log_decay)
    scale_in = jnp.sqrt(-jnp.expm1(2.0 * log_decay))
    signal = rec_value.astype(F32)
    before_state = prev_state.astype(F32)
    rec_state = (decay * before_state + scale_in * input_gate * signal).astype(BF16)
    value_by = scale_in * input_gate
    input_by = value_by * signal * (1.0 - input_gate)
    decay_part = decay * before_state - input_gate * signal * decay * decay / scale_in
    rate_by = decay_part * (-decay_scale * decay_speed) * rate_gate * (1.0 - rate_gate)

    local, through, last = chain_within(mix_grad, out_proj, rec_state, decay, n_sp)
    last = lax.all_to_all(last, SP, 0, 0, tiled=True)
    here = lax.axis_index(SP).reshape(1).astype(jnp.int32)
    out_proj_grad, rec_value_grad, input_pre_grad, rate_pre_grad = finish(
        here, last, local, through, value_by, input_by, rate_by
    )
    return (
        dgu_sum[0][None],
        dgu_sum[1][None],
        d_down[None],
        out_proj_grad,
        rec_value_grad,
        rate_pre_grad,
        input_pre_grad,
    )


def solution(mesh):
    finer = Mesh(mesh.devices.reshape(8, 4, 8, 2), ("z", "x", "y", "c"))
    grid = P(SP, TP)
    return jax.shard_map(
        per_device,
        mesh=finer,
        in_specs=(
            grid,
            grid,
            P(SP, None),
            P(SP, None),
            P(SP, None, TP),
            P(SP, None, TP),
            P(SP, TP, None),
            P(TP, None),
            grid,
            grid,
            grid,
            grid,
            P(TP),
        ),
        out_specs=(P(SP, None, TP), P(SP, None, TP), P(SP, TP, None), grid, grid, grid, grid),
        check_vma=False,
    )
```

```python
import functools

import jax
import jax.numpy as jnp
from jax import lax
from jax.experimental import pallas as pl
from jax.experimental.pallas import tpu as pltpu
from jax.sharding import Mesh
from jax.sharding import PartitionSpec as P

SP = ("z", "x")
TP = ("y", "c")
F32 = jnp.float32
BF16 = jnp.bfloat16
decay_scale = 8.0

SMEM = pl.BlockSpec(memory_space=pltpu.SMEM)
VMEM = pl.BlockSpec(memory_space=pltpu.VMEM)


def whole(shape, dtype):
    return jax.ShapeDtypeStruct(shape, dtype)


def call(body, out, *operands, scalars=0, scratch=(), loose=(), kept=()):
    held = [
        o if i < scalars or i in loose else pltpu.with_memory_space_constraint(o, pltpu.VMEM)
        for i, o in enumerate(operands)
    ]
    outs = [(pltpu.VMEM if i in kept else pltpu.HBM)(o.shape, o.dtype) for i, o in enumerate(out)]
    got = pl.pallas_call(
        body,
        out_shape=tuple(outs),
        in_specs=[SMEM] * scalars + [VMEM] * (len(operands) - scalars),
        out_specs=tuple([VMEM] * len(outs)),
        scratch_shapes=list(scratch),
        compiler_params=pltpu.CompilerParams(vmem_limit_bytes=16 * 2**20),
    )(*held)
    return got if len(out) > 1 else got[0]


def dot(a, b, dims):
    return lax.dot_general(a, b, (dims, ((), ())), preferred_element_type=F32)


def iota(shape, dim):
    return lax.broadcasted_iota(jnp.int32, shape, dim)


def route_body(core, routes, weights, pick, choose, scale, *, experts, half):
    me = core[0]
    count, tokens = routes.shape
    slots = experts * (half + 1)
    here = [iota((experts, tokens), 0) == routes[k : k + 1, :] for k in range(count)]
    named = functools.reduce(jnp.logical_or, here)
    earlier = iota((tokens, tokens), 0) < iota((tokens, tokens), 1)
    before = dot(
        jnp.where(named, 1.0, 0.0).astype(BF16), jnp.where(earlier, 1.0, 0.0).astype(BF16), ((1,), (0,))
    )
    back, mine = [], []
    for k in range(count):
        rank = jnp.sum(jnp.where(here[k], before, 0.0), axis=0, keepdims=True).astype(jnp.int32)
        name = routes[k : k + 1, :]
        back.append(name * 16 + rank + jnp.where(rank >= half, 8 - half, 0))
        at = rank - me * half
        mine.append(jnp.where((at >= 0) & (at < half), name * (half + 1) + at, -1))
    hit = functools.reduce(jnp.logical_or, [iota(pick.shape, 0) == b for b in back])
    pick[...] = jnp.where(hit, 1.0, 0.0).astype(BF16)
    row = iota((slots, tokens), 0)
    hits = [row == m for m in mine]
    scale[...] = sum(
        jnp.sum(jnp.where(h, weights[k : k + 1, :], 0.0), axis=1, keepdims=True)
        for k, h in enumerate(hits)
    )
    choose[...] = jnp.where(functools.reduce(jnp.logical_or, hits), 1.0, 0.0).astype(BF16)


def route_slots(core, routes, weights, experts, half):
    tokens, slots = routes.shape[1], experts * (half + 1)
    out = (whole((experts * 16, tokens), BF16), whole((slots, tokens), BF16), whole((slots, 1), F32))
    body = functools.partial(route_body, experts=experts, half=half)
    return call(body, out, core, routes, weights, scalars=1, loose=(1, 2), kept=(1, 2))


def fill_body(core, choose, scale, mine, peer, send, rows):
    slots = choose.shape[0]
    for a in range(2):
        for c in range(2):
            r = dot(choose[...], jnp.where(core[0] == c, mine[a], peer[a]), ((1,), (0,)))
            rows[pl.ds(2 * a + c, slots, stride=4), :] = scale[...] * r if a else r
    send[...] = rows[...].astype(BF16)


def fill_slots(core, choose, scale, mine, peer):
    shape = (choose.shape[0] * 4, mine.shape[-1])
    out = (whole(shape, BF16),)
    scratch = [pltpu.VMEM(shape, F32)]
    return call(fill_body, out, core, choose, scale, mine, peer, scalars=1, scratch=scratch)


def sort_body(recv, pieces, rows, *, half):
    slots = recv.shape[0] // 4
    kept = pieces.shape[1]
    rows[...] = recv[...].astype(F32)
    r, c = iota((kept, slots), 0), iota((kept, slots), 1)
    block = (c * (65536 // (half + 1) + 1)) >> 16
    hit = (c - block == r) & (c - block * (half + 1) < half)
    keep = jnp.where(hit, 1.0, 0.0).astype(BF16)
    for q in range(4):
        v = rows[pl.ds(q, slots, stride=4), :].astype(BF16)
        pieces[q] = dot(keep, v, ((1,), (0,))).astype(BF16)


def sort_pieces(recv, half):
    kept = recv.shape[0] // 4 // (half + 1) * half
    out = (whole((4, kept, recv.shape[1]), BF16),)
    body = functools.partial(sort_body, half=half)
    return call(body, out, recv, scratch=[pltpu.VMEM(recv.shape, F32)], kept=(0,))


OFFSETS = (0, -1, 1, -2, 2, 4, 3, 5)


def shards(chip, blocks, n_y):
    for off, ref in zip(OFFSETS, blocks):
        y = lax.rem(chip + off % n_y, n_y)
        yield y, jnp.concatenate([ref[0], ref[1]], axis=1), jnp.concatenate([ref[2], ref[3]], axis=1)


def expert_body(chip, *refs):
    blocks, (wgu_peer, wg, wu, wd, wd_peer, gu_grad, hidden, part) = refs[:8], refs[8:]
    n_y = part.shape[0]
    fw = wd.shape[0]
    rows, hid = hidden.shape
    acc = jnp.zeros((rows, 2 * hid), F32)
    back = jnp.zeros((rows, hid), F32)

    def weights(y):
        at = pl.ds(pl.multiple_of(y * 2 * fw, 2 * fw), 2 * fw)
        return jnp.concatenate([wg[at, :], wgu_peer[0, at, :], wu[at, :], wgu_peer[1, at, :]], axis=1), at

    for y, x_in, x_cot in shards(chip[0], blocks, n_y):
        w, at = weights(y)
        acc = acc + dot(x_in, w, ((1,), (0,)))
        back = back + dot(x_cot, jnp.concatenate([wd[:, at], wd_peer[:, at]], axis=0), ((1,), (1,)))
    gate, up = acc[:, :hid], acc[:, hid:]
    squash = jax.nn.sigmoid(gate)
    silu = gate * squash
    hidden[...] = (silu * up).astype(BF16)
    g_grad = (back * up * squash * (1.0 + gate * (1.0 - squash))).astype(BF16)
    u_grad = (back * silu).astype(BF16)
    grads = jnp.concatenate([g_grad, u_grad], axis=1)
    gu_grad[...] = grads
    for y in range(n_y):
        w, _ = weights(y)
        r = dot(grads, w, ((1,), (1,))).astype(BF16)
        part[y, 0] = r[:, :fw]
        part[y, 1] = r[:, fw:]


def expert_rows_grad(chip, blocks, wgu_peer, wg, wu, wd, wd_peer, n_y):
    rows, fw = blocks[0].shape[1:]
    hid = 2 * wg.shape[1]

    out = (whole((rows, 2 * hid), BF16), whole((rows, hid), BF16), whole((n_y, 2, rows, fw), BF16))
    weights = (wgu_peer, wg, wu, wd, wd_peer)
    return call(expert_body, out, chip, *blocks, *weights, scalars=1)


def weight_body(chip, *refs):
    blocks, (gu_grad, hidden, dgu, dgu_send, dd, dd_send) = refs[:8], refs[8:]
    fw = dd.shape[0]
    hid = hidden.shape[1]
    n_y = dd.shape[1] // (2 * fw)
    for y, x_in, x_cot in shards(chip[0], blocks, n_y):
        at = pl.ds(pl.multiple_of(y * 2 * fw, 2 * fw), 2 * fw)
        r = dot(x_in, gu_grad[...], ((0,), (0,))).astype(BF16)
        for i in range(2):
            dgu[i, at, :] = r[:, i * hid : i * hid + fw]
            dgu_send[i, at, :] = r[:, i * hid + fw : (i + 1) * hid]
        r = dot(hidden[...], x_cot, ((0,), (0,))).astype(BF16)
        dd[:, at] = r[:fw]
        dd_send[:, at] = r[fw:]


def expert_weight_grads(chip, blocks, gu_grad, hidden, d):
    fw = blocks[0].shape[2]
    out = (whole((2, d, fw), BF16),) * 2 + (whole((fw, d), BF16),) * 2
    return call(weight_body, out, chip, *blocks, gu_grad, hidden, scalars=1, loose=(9, 10))


def add_body(parts, out, *, half):
    n_y, n_h, rows, _ = parts.shape
    j, r = iota((out.shape[0], rows), 0), iota((out.shape[0], rows), 1)
    slot = j & 7
    source = (j >> 4) * half + slot
    total = 0.0
    for h in range(n_h):
        s = parts[0, h].astype(F32)
        for y in range(1, n_y):
            s = s + parts[y, h].astype(F32)
        hit = (source == r) & (slot < half) & (((j >> 3) & 1) == h)
        total = total + dot(jnp.where(hit, 1.0, 0.0).astype(BF16), s.astype(BF16), ((1,), (0,)))
    out[...] = total.astype(BF16)


def add_parts(parts, blocks, half):
    out = (whole((blocks * 16, parts.shape[3]), BF16),)
    return call(functools.partial(add_body, half=half), out, parts)


def later(v, step, fill):
    return jnp.concatenate([v[step:], jnp.full((step, v.shape[1]), fill, v.dtype)], axis=0)


def in_three(v):
    hi = v.astype(BF16)
    mid = (v - hi.astype(F32)).astype(BF16)
    lo = (v - hi.astype(F32) - mid.astype(F32)).astype(BF16)
    return [p.astype(F32) for p in (hi, mid, lo)]


def chain_body(mix, out_proj, rec_state, decay, local, through, last):
    n_sp, width = last.shape[0], last.shape[2]
    keep = mix.shape[1] // n_sp
    proj = dot(mix[...], rec_state[...], ((0,), (0,))).astype(BF16)
    for k in range(n_sp):
        last[k, :keep, :] = proj[k * keep : (k + 1) * keep, :]
    grad = dot(mix[...], out_proj[...], ((1,), (1,)))
    mult = later(decay[...], 1, 1.0)
    step = 1
    while step < grad.shape[0]:
        grad = grad + mult * later(grad, step, 0.0)
        mult = mult * later(mult, step, 1.0)
        step *= 2
    local[...] = grad
    through[...] = mult
    first = decay[0:1, :]
    row = iota((last.shape[1] - keep, width), 0)
    chain = jnp.zeros(row.shape, F32)
    for i, piece in enumerate(in_three(first * mult[0:1, :]) + in_three(first * grad[0:1, :])):
        chain = jnp.where(row == i, piece, chain)
    chain = chain.astype(BF16)
    for k in range(n_sp):
        last[k, keep:, :] = chain


def chain_within(mix, out_proj, rec_state, decay, n_sp):
    tokens, width = decay.shape
    last = whole((n_sp, mix.shape[1] // n_sp + 8, width), BF16)
    out = (whole((tokens, width), F32),) * 2 + (last,)
    return call(chain_body, out, mix, out_proj, rec_state, decay, kept=(0, 1))


def finish_body(here, last, local, through, value_by, input_by, rate_by, proj, value, inp, rate):
    n_sp = last.shape[0]
    keep = proj.shape[0]
    incoming = jnp.zeros((1, last.shape[2]), F32)
    for k in reversed(range(n_sp)):
        c = last[k, keep:, :].astype(F32)
        mult = (c[2:3] + c[1:2]) + c[0:1]
        add = (c[5:6] + c[4:5]) + c[3:4]
        incoming = jnp.where(k > here[0], add + mult * incoming, incoming)
    carried = local[...] + through[...] * incoming
    value[...] = (carried * value_by[...]).astype(BF16)
    inp[...] = (carried * input_by[...]).astype(BF16)
    rate[...] = (carried * rate_by[...]).astype(BF16)
    total = last[0, :keep, :].astype(F32)
    for k in range(1, n_sp):
        total = total + last[k, :keep, :].astype(F32)
    proj[...] = total


def finish(here, last, local, through, value_by, input_by, rate_by):
    grid = whole(local.shape, BF16)
    out = (whole((last.shape[1] - 8, last.shape[2]), F32), grid, grid, grid)
    return call(finish_body, out, here, last, local, through, value_by, input_by, rate_by, scalars=1)


def per_device(
    ffn_input,
    out_grad,
    routes,
    route_weight,
    gate_w,
    up_w,
    down_w,
    out_proj,
    rec_value,
    rate_pre,
    input_pre,
    prev_state,
    decay_param,
):
    n_sp, n_y = lax.axis_size(SP), lax.axis_size("y")
    tok, count = routes.shape
    half = 5 * count * tok // (8 * n_sp)
    fw = ffn_input.shape[1]
    d = gate_w.shape[1]
    chip = lax.axis_index("y").reshape(1).astype(jnp.int32)
    core = lax.axis_index("c").reshape(1).astype(jnp.int32)

    def over_y(v, step):
        return lax.ppermute(v, "y", [(i, (i + step) % n_y) for i in range(n_y)])

    def over_cores(v):
        return lax.ppermute(v, "c", [(0, 1), (1, 0)])

    own = jnp.stack([ffn_input, out_grad])
    far = over_y(own, n_y // 2)
    peer = over_cores(own)
    pick, choose, scale = route_slots(core, routes.T, route_weight.T, n_sp, half)

    def dispatch(mine, other):
        send = fill_slots(core, choose, scale, mine, other)
        recv = lax.all_to_all(send.reshape(n_sp, -1, fw), SP, 0, 0, tiled=True).reshape(send.shape)
        return send, sort_pieces(recv, half)

    near_send, near = dispatch(own, peer)
    far_peer = over_cores(far)
    _, beyond = dispatch(far, far_peer)

    _, late_gate, late_up, late_down = lax.optimization_barrier((near_send, gate_w, up_w, down_w))
    wgu = jnp.concatenate([late_gate, late_up], axis=0)
    wgu_peer = over_cores(wgu)
    wd_peer = over_cores(late_down[0])
    near_blocks = [over_y(near, step) for step in (1, -1, 2, -2)]
    far_blocks = [over_y(beyond, step) for step in (1, -1)]
    blocks = (near, *near_blocks, beyond, *far_blocks)

    gu_grad, hidden, part = expert_rows_grad(
        chip, blocks, wgu_peer, late_gate[0], late_up[0], late_down[0], wd_peer, n_y
    )
    arrived = lax.all_to_all(part.reshape(2 * n_y, *part.shape[2:]), TP, 0, 0, tiled=True)
    back = add_parts(arrived.reshape(part.shape), n_sp, half)
    returned = lax.all_to_all(back.reshape(n_sp, 16, fw), SP, 0, 0, tiled=True).reshape(back.shape)
    dgu, dgu_send, dd, dd_send = expert_weight_grads(chip, blocks, gu_grad, hidden, d)
    dgu_peer = over_cores(dgu_send)
    dd_peer = over_cores(dd_send)
    dgu_sum = (dgu.astype(F32) + dgu_peer.astype(F32)).astype(BF16)
    d_down = (dd.astype(F32) + dd_peer.astype(F32)).astype(BF16)
    own_grad = (dot(pick, returned, ((0,), (0,))) + out_grad.astype(F32)).astype(BF16)
    mix_grad = lax.all_gather(own_grad, TP, axis=1, tiled=True)

    rate_gate = jax.nn.sigmoid(rate_pre.astype(F32))
    input_gate = jax.nn.sigmoid(input_pre.astype(F32))
    decay_speed = jax.nn.softplus(-decay_param)[None, :]
    log_decay = -decay_scale * rate_gate * decay_speed
    decay = jnp.exp(log_decay)
    scale_in = jnp.sqrt(-jnp.expm1(2.0 * log_decay))
    signal = rec_value.astype(F32)
    before_state = prev_state.astype(F32)
    rec_state = (decay * before_state + scale_in * input_gate * signal).astype(BF16)
    value_by = scale_in * input_gate
    input_by = value_by * signal * (1.0 - input_gate)
    decay_part = decay * before_state - input_gate * signal * decay * decay / scale_in
    rate_by = decay_part * (-decay_scale * decay_speed) * rate_gate * (1.0 - rate_gate)

    local, through, last = chain_within(mix_grad, out_proj, rec_state, decay, n_sp)
    last = lax.all_to_all(last, SP, 0, 0, tiled=True)
    here = lax.axis_index(SP).reshape(1).astype(jnp.int32)
    out_proj_grad, rec_value_grad, input_pre_grad, rate_pre_grad = finish(
        here, last, local, through, value_by, input_by, rate_by
    )
    return (
        dgu_sum[0][None],
        dgu_sum[1][None],
        d_down[None],
        out_proj_grad,
        rec_value_grad,
        rate_pre_grad,
        input_pre_grad,
    )


def solution(mesh):
    finer = Mesh(mesh.devices.reshape(8, 4, 8, 2), ("z", "x", "y", "c"))
    grid = P(SP, TP)
    return jax.shard_map(
        per_device,
        mesh=finer,
        in_specs=(
            grid,
            grid,
            P(SP, None),
            P(SP, None),
            P(SP, None, TP),
            P(SP, None, TP),
            P(SP, TP, None),
            P(TP, None),
            grid,
            grid,
            grid,
            grid,
            P(TP),
        ),
        out_specs=(P(SP, None, TP), P(SP, None, TP), P(SP, TP, None), grid, grid, grid, grid),
        check_vma=False,
    )
```

```python
import functools

import jax
import jax.numpy as jnp
from jax import lax
from jax.experimental import pallas as pl
from jax.experimental.pallas import tpu as pltpu
from jax.sharding import Mesh
from jax.sharding import PartitionSpec as P

SP = ("z", "x")
TP = ("y", "c")
F32 = jnp.float32
BF16 = jnp.bfloat16
decay_scale = 8.0

SMEM = pl.BlockSpec(memory_space=pltpu.SMEM)
VMEM = pl.BlockSpec(memory_space=pltpu.VMEM)


def whole(shape, dtype):
    return jax.ShapeDtypeStruct(shape, dtype)


def call(body, out, *operands, scalars=0, scratch=(), loose=(), kept=()):
    held = [
        o if i < scalars or i in loose else pltpu.with_memory_space_constraint(o, pltpu.VMEM)
        for i, o in enumerate(operands)
    ]
    outs = [(pltpu.VMEM if i in kept else pltpu.HBM)(o.shape, o.dtype) for i, o in enumerate(out)]
    got = pl.pallas_call(
        body,
        out_shape=tuple(outs),
        in_specs=[SMEM] * scalars + [VMEM] * (len(operands) - scalars),
        out_specs=tuple([VMEM] * len(outs)),
        scratch_shapes=list(scratch),
        compiler_params=pltpu.CompilerParams(vmem_limit_bytes=16 * 2**20),
    )(*held)
    return got if len(out) > 1 else got[0]


def dot(a, b, dims):
    return lax.dot_general(a, b, (dims, ((), ())), preferred_element_type=F32)


def iota(shape, dim):
    return lax.broadcasted_iota(jnp.int32, shape, dim)


def route_body(core, routes, weights, pick, choose, scale, *, experts, half):
    me = core[0]
    count, tokens = routes.shape
    slots = experts * half
    here = [iota((experts, tokens), 0) == routes[k : k + 1, :] for k in range(count)]
    named = functools.reduce(jnp.logical_or, here)
    earlier = iota((tokens, tokens), 0) < iota((tokens, tokens), 1)
    before = dot(
        jnp.where(named, 1.0, 0.0).astype(BF16), jnp.where(earlier, 1.0, 0.0).astype(BF16), ((1,), (0,))
    )
    back, mine = [], []
    for k in range(count):
        rank = jnp.sum(jnp.where(here[k], before, 0.0), axis=0, keepdims=True).astype(jnp.int32)
        name = routes[k : k + 1, :]
        back.append(name * 16 + rank + jnp.where(rank >= half, 8 - half, 0))
        at = rank - me * half
        mine.append(jnp.where((at >= 0) & (at < half), name * half + at, -1))
    hit = functools.reduce(jnp.logical_or, [iota(pick.shape, 0) == b for b in back])
    pick[...] = jnp.where(hit, 1.0, 0.0).astype(BF16)
    row = iota((slots, tokens), 0)
    hits = [row == m for m in mine]
    scale[...] = sum(
        jnp.sum(jnp.where(h, weights[k : k + 1, :], 0.0), axis=1, keepdims=True)
        for k, h in enumerate(hits)
    )
    choose[...] = jnp.where(functools.reduce(jnp.logical_or, hits), 1.0, 0.0).astype(BF16)


def route_slots(core, routes, weights, experts, half):
    tokens, slots = routes.shape[1], experts * half
    out = (whole((experts * 16, tokens), BF16), whole((slots, tokens), BF16), whole((slots, 1), F32))
    body = functools.partial(route_body, experts=experts, half=half)
    return call(body, out, core, routes, weights, scalars=1, loose=(1, 2), kept=(1, 2))


def fill_body(core, choose, scale, mine, peer, send, rows):
    me = core[0]
    slots = choose.shape[0]
    for a in range(2):
        for n in range(2):
            for c in range(2):
                x = jnp.where(me == c, mine[n, a], peer[n, a])
                r = dot(choose[...], x, ((1,), (0,)))
                rows[pl.ds(4 * a + 2 * n + c, slots, stride=8), :] = scale[...] * r if a else r
    send[...] = rows[...].astype(BF16)


def fill_slots(core, choose, scale, mine, peer):
    fw = mine.shape[-1]
    total = choose.shape[0] * 8
    out = (whole((total, fw), BF16),)
    scratch = [pltpu.VMEM((total, fw), F32)]
    return call(fill_body, out, core, choose, scale, mine, peer, scalars=1, scratch=scratch)


def sort_body(recv, both, near, rows):
    slots = recv.shape[0] // 8
    rows[...] = recv[...].astype(F32)
    for a in range(2):
        for n in range(2):
            for c in range(2):
                v = rows[pl.ds(4 * a + 2 * n + c, slots, stride=8), :].astype(BF16)
                both[n, 2 * a + c] = v
                if n == 0:
                    near[2 * a + c] = v


def sort_pieces(recv):
    slots, fw = recv.shape[0] // 8, recv.shape[1]
    out = (whole((2, 4, slots, fw), BF16), whole((4, slots, fw), BF16))
    return call(sort_body, out, recv, scratch=[pltpu.VMEM(recv.shape, F32)], kept=(0, 1))


def shards(chip, both, f1, b1, f2, b2, n_y):
    found = []
    for off, ref in ((0, both), (n_y - 1, f1), (1, b1)):
        for n in range(2):
            found.append((off + 4 * n, [ref[n, i] for i in range(4)]))
    for off, ref in ((n_y - 2, f2), (2, b2)):
        found.append((off, [ref[i] for i in range(4)]))
    for off, p in found:
        y = lax.rem(chip + off, n_y)
        yield y, jnp.concatenate(p[:2], axis=1), jnp.concatenate(p[2:], axis=1)


def expert_body(chip, both, f1, b1, f2, b2, wgu_peer, wg, wu, wd, wd_peer, gu_grad, hidden, part):
    n_y = part.shape[0]
    fw = wd.shape[0]
    rows, hid = hidden.shape
    acc = jnp.zeros((rows, 2 * hid), F32)
    back = jnp.zeros((rows, hid), F32)

    def weights(y):
        at = pl.ds(pl.multiple_of(y * 2 * fw, 2 * fw), 2 * fw)
        return jnp.concatenate([wg[at, :], wgu_peer[0, at, :], wu[at, :], wgu_peer[1, at, :]], axis=1), at

    for y, x_in, x_cot in shards(chip[0], both, f1, b1, f2, b2, n_y):
        w, at = weights(y)
        acc = acc + dot(x_in, w, ((1,), (0,)))
        back = back + dot(x_cot, jnp.concatenate([wd[:, at], wd_peer[:, at]], axis=0), ((1,), (1,)))
    gate, up = acc[:, :hid], acc[:, hid:]
    squash = jax.nn.sigmoid(gate)
    silu = gate * squash
    hidden[...] = (silu * up).astype(BF16)
    g_grad = (back * up * squash * (1.0 + gate * (1.0 - squash))).astype(BF16)
    u_grad = (back * silu).astype(BF16)
    grads = jnp.concatenate([g_grad, u_grad], axis=1)
    gu_grad[...] = grads
    for y in range(n_y):
        w, _ = weights(y)
        r = dot(grads, w, ((1,), (1,))).astype(BF16)
        part[y, 0] = r[:, :fw]
        part[y, 1] = r[:, fw:]


def expert_rows_grad(chip, blocks, wgu_peer, wg, wu, wd, wd_peer, n_y):
    rows, fw = blocks[0].shape[2:]
    hid = 2 * wg.shape[1]

    out = (whole((rows, 2 * hid), BF16), whole((rows, hid), BF16), whole((n_y, 2, rows, fw), BF16))
    weights = (wgu_peer, wg, wu, wd, wd_peer)
    return call(expert_body, out, chip, *blocks, *weights, scalars=1)


def weight_body(chip, both, f1, b1, f2, b2, gu_grad, hidden, dgu, dgu_send, dd, dd_send):
    fw = dd.shape[0]
    hid = hidden.shape[1]
    n_y = dd.shape[1] // (2 * fw)
    for y, x_in, x_cot in shards(chip[0], both, f1, b1, f2, b2, n_y):
        at = pl.ds(pl.multiple_of(y * 2 * fw, 2 * fw), 2 * fw)
        r = dot(x_in, gu_grad[...], ((0,), (0,))).astype(BF16)
        for i in range(2):
            dgu[i, at, :] = r[:, i * hid : i * hid + fw]
            dgu_send[i, at, :] = r[:, i * hid + fw : (i + 1) * hid]
        r = dot(hidden[...], x_cot, ((0,), (0,))).astype(BF16)
        dd[:, at] = r[:fw]
        dd_send[:, at] = r[fw:]


def expert_weight_grads(chip, blocks, gu_grad, hidden, d):
    fw = blocks[0].shape[3]
    out = (whole((2, d, fw), BF16),) * 2 + (whole((fw, d), BF16),) * 2
    return call(weight_body, out, chip, *blocks, gu_grad, hidden, scalars=1, loose=(6, 7))


def add_body(parts, out, *, half):
    n_y, n_h, rows, _ = parts.shape
    j, r = iota((out.shape[0], rows), 0), iota((out.shape[0], rows), 1)
    slot = j & 7
    source = (j >> 4) * half + slot
    total = 0.0
    for h in range(n_h):
        s = parts[0, h].astype(F32)
        for y in range(1, n_y):
            s = s + parts[y, h].astype(F32)
        hit = (source == r) & (slot < half) & (((j >> 3) & 1) == h)
        total = total + dot(jnp.where(hit, 1.0, 0.0).astype(BF16), s.astype(BF16), ((1,), (0,)))
    out[...] = total.astype(BF16)


def add_parts(parts, blocks, half):
    out = (whole((blocks * 16, parts.shape[3]), BF16),)
    return call(functools.partial(add_body, half=half), out, parts, kept=(0,))


def later(v, step, fill):
    return jnp.concatenate([v[step:], jnp.full((step, v.shape[1]), fill, v.dtype)], axis=0)


def in_three(v):
    hi = v.astype(BF16)
    mid = (v - hi.astype(F32)).astype(BF16)
    lo = (v - hi.astype(F32) - mid.astype(F32)).astype(BF16)
    return [p.astype(F32) for p in (hi, mid, lo)]


def chain_body(mix, out_proj, rec_state, decay, local, through, last):
    n_sp, width = last.shape[0], last.shape[2]
    keep = mix.shape[1] // n_sp
    proj = dot(mix[...], rec_state[...], ((0,), (0,))).astype(BF16)
    for k in range(n_sp):
        last[k, :keep, :] = proj[k * keep : (k + 1) * keep, :]
    grad = dot(mix[...], out_proj[...], ((1,), (1,)))
    mult = later(decay[...], 1, 1.0)
    step = 1
    while step < grad.shape[0]:
        grad = grad + mult * later(grad, step, 0.0)
        mult = mult * later(mult, step, 1.0)
        step *= 2
    local[...] = grad
    through[...] = mult
    first = decay[0:1, :]
    row = iota((last.shape[1] - keep, width), 0)
    chain = jnp.zeros(row.shape, F32)
    for i, piece in enumerate(in_three(first * mult[0:1, :]) + in_three(first * grad[0:1, :])):
        chain = jnp.where(row == i, piece, chain)
    chain = chain.astype(BF16)
    for k in range(n_sp):
        last[k, keep:, :] = chain


def chain_within(mix, out_proj, rec_state, decay, n_sp):
    tokens, width = decay.shape
    last = whole((n_sp, mix.shape[1] // n_sp + 8, width), BF16)
    out = (whole((tokens, width), F32),) * 2 + (last,)
    return call(chain_body, out, mix, out_proj, rec_state, decay, kept=(0, 1, 2))


def finish_body(here, last, local, through, value_by, input_by, rate_by, proj, value, inp, rate):
    n_sp = last.shape[0]
    keep = proj.shape[0]
    incoming = jnp.zeros((1, last.shape[2]), F32)
    for k in reversed(range(n_sp)):
        c = last[k, keep:, :].astype(F32)
        mult = (c[2:3] + c[1:2]) + c[0:1]
        add = (c[5:6] + c[4:5]) + c[3:4]
        incoming = jnp.where(k > here[0], add + mult * incoming, incoming)
    carried = local[...] + through[...] * incoming
    value[...] = (carried * value_by[...]).astype(BF16)
    inp[...] = (carried * input_by[...]).astype(BF16)
    rate[...] = (carried * rate_by[...]).astype(BF16)
    total = last[0, :keep, :].astype(F32)
    for k in range(1, n_sp):
        total = total + last[k, :keep, :].astype(F32)
    proj[...] = total


def finish(here, last, local, through, value_by, input_by, rate_by):
    grid = whole(local.shape, BF16)
    out = (whole((last.shape[1] - 8, last.shape[2]), F32), grid, grid, grid)
    return call(finish_body, out, here, last, local, through, value_by, input_by, rate_by, scalars=1)


def per_device(
    ffn_input,
    out_grad,
    routes,
    route_weight,
    gate_w,
    up_w,
    down_w,
    out_proj,
    rec_value,
    rate_pre,
    input_pre,
    prev_state,
    decay_param,
):
    n_sp, n_y = lax.axis_size(SP), lax.axis_size("y")
    tok, count = routes.shape
    half = 5 * count * tok // (8 * n_sp)
    fw = ffn_input.shape[1]
    d = gate_w.shape[1]
    chip = lax.axis_index("y").reshape(1).astype(jnp.int32)
    core = lax.axis_index("c").reshape(1).astype(jnp.int32)

    def over_y(v, step):
        return lax.ppermute(v, "y", [(i, (i + step) % n_y) for i in range(n_y)])

    def over_cores(v):
        return lax.ppermute(v, "c", [(0, 1), (1, 0)])

    own = jnp.stack([ffn_input, out_grad])
    far = over_y(own, n_y // 2)
    mine = jnp.stack([own, far])
    peer = over_cores(mine)
    pick, choose, scale = route_slots(core, routes.T, route_weight.T, n_sp, half)
    send = fill_slots(core, choose, scale, mine, peer)

    send, late_gate, late_up, late_down = lax.optimization_barrier((send, gate_w, up_w, down_w))
    wgu = jnp.concatenate([late_gate, late_up], axis=0)
    wgu_peer = over_cores(wgu)
    wd_peer = over_cores(late_down[0])
    recv = lax.all_to_all(send.reshape(n_sp, -1, fw), SP, 0, 0, tiled=True).reshape(send.shape)
    both, near = sort_pieces(recv)
    blocks = (both, over_y(both, 1), over_y(both, -1), over_y(near, 2), over_y(near, -2))

    gu_grad, hidden, part = expert_rows_grad(
        chip, blocks, wgu_peer, late_gate[0], late_up[0], late_down[0], wd_peer, n_y
    )
    rate_gate = jax.nn.sigmoid(rate_pre.astype(F32))
    input_gate = jax.nn.sigmoid(input_pre.astype(F32))
    decay_speed = jax.nn.softplus(-decay_param)[None, :]
    log_decay = -decay_scale * rate_gate * decay_speed
    decay = jnp.exp(log_decay)
    scale_in = jnp.sqrt(-jnp.expm1(2.0 * log_decay))
    signal = rec_value.astype(F32)
    before_state = prev_state.astype(F32)
    rec_state = (decay * before_state + scale_in * input_gate * signal).astype(BF16)
    value_by = scale_in * input_gate
    input_by = value_by * signal * (1.0 - input_gate)
    decay_part = decay * before_state - input_gate * signal * decay * decay / scale_in
    rate_by = decay_part * (-decay_scale * decay_speed) * rate_gate * (1.0 - rate_gate)
    here = lax.axis_index(SP).reshape(1).astype(jnp.int32)
    part, here = lax.optimization_barrier((part, here))
    arrived = lax.all_to_all(part.reshape(2 * n_y, *part.shape[2:]), TP, 0, 0, tiled=True)
    back = add_parts(arrived.reshape(part.shape), n_sp, half)
    returned = lax.all_to_all(back.reshape(n_sp, 16, fw), SP, 0, 0, tiled=True).reshape(back.shape)
    dgu, dgu_send, dd, dd_send = expert_weight_grads(chip, blocks, gu_grad, hidden, d)
    dgu_peer = over_cores(dgu_send)
    dd_peer = over_cores(dd_send)
    d_gate, d_up = [(dgu[i].astype(F32) + dgu_peer[i].astype(F32)).astype(BF16)[None] for i in range(2)]
    d_down = (dd.astype(F32) + dd_peer.astype(F32)).astype(BF16)[None]
    own_grad = (dot(pick, returned, ((0,), (0,))) + out_grad.astype(F32)).astype(BF16)
    mix_grad = lax.all_gather(own_grad, TP, axis=1, tiled=True)

    local, through, last = chain_within(mix_grad, out_proj, rec_state, decay, n_sp)
    last = lax.all_to_all(last, SP, 0, 0, tiled=True)
    out_proj_grad, rec_value_grad, input_pre_grad, rate_pre_grad = finish(
        here, last, local, through, value_by, input_by, rate_by
    )
    return (
        d_gate,
        d_up,
        d_down,
        out_proj_grad,
        rec_value_grad,
        rate_pre_grad,
        input_pre_grad,
    )


def solution(mesh):
    finer = Mesh(mesh.devices.reshape(8, 4, 8, 2), ("z", "x", "y", "c"))
    grid = P(SP, TP)
    return jax.shard_map(
        per_device,
        mesh=finer,
        in_specs=(
            grid,
            grid,
            P(SP, None),
            P(SP, None),
            P(SP, None, TP),
            P(SP, None, TP),
            P(SP, TP, None),
            P(TP, None),
            grid,
            grid,
            grid,
            grid,
            P(TP),
        ),
        out_specs=(P(SP, None, TP), P(SP, None, TP), P(SP, TP, None), grid, grid, grid, grid),
        check_vma=False,
    )
```

```python
import functools

import jax
import jax.numpy as jnp
from jax import lax
from jax.experimental import pallas as pl
from jax.experimental.pallas import tpu as pltpu
from jax.sharding import Mesh
from jax.sharding import PartitionSpec as P

SP = ("z", "x")
TP = ("y", "c")
F32 = jnp.float32
BF16 = jnp.bfloat16
decay_scale = 8.0

SMEM = pl.BlockSpec(memory_space=pltpu.SMEM)
VMEM = pl.BlockSpec(memory_space=pltpu.VMEM)


def whole(shape, dtype):
    return jax.ShapeDtypeStruct(shape, dtype)


def call(body, out, *operands, scalars=0, scratch=(), loose=(), kept=()):
    held = [
        o if i < scalars or i in loose else pltpu.with_memory_space_constraint(o, pltpu.VMEM)
        for i, o in enumerate(operands)
    ]
    outs = [(pltpu.VMEM if i in kept else pltpu.HBM)(o.shape, o.dtype) for i, o in enumerate(out)]
    got = pl.pallas_call(
        body,
        out_shape=tuple(outs),
        in_specs=[SMEM] * scalars + [VMEM] * (len(operands) - scalars),
        out_specs=tuple([VMEM] * len(outs)),
        scratch_shapes=list(scratch),
        compiler_params=pltpu.CompilerParams(vmem_limit_bytes=16 * 2**20),
    )(*held)
    return got if len(out) > 1 else got[0]


def dot(a, b, dims):
    return lax.dot_general(a, b, (dims, ((), ())), preferred_element_type=F32)


def iota(shape, dim):
    return lax.broadcasted_iota(jnp.int32, shape, dim)


def route_body(core, routes, weights, pick, choose, scale, *, experts, half):
    me = core[0]
    count, tokens = routes.shape
    slots = experts * half
    here = [iota((experts, tokens), 0) == routes[k : k + 1, :] for k in range(count)]
    named = functools.reduce(jnp.logical_or, here)
    earlier = iota((tokens, tokens), 0) < iota((tokens, tokens), 1)
    before = dot(
        jnp.where(named, 1.0, 0.0).astype(BF16), jnp.where(earlier, 1.0, 0.0).astype(BF16), ((1,), (0,))
    )
    back, mine = [], []
    for k in range(count):
        rank = jnp.sum(jnp.where(here[k], before, 0.0), axis=0, keepdims=True).astype(jnp.int32)
        name = routes[k : k + 1, :]
        back.append(name * 16 + rank + jnp.where(rank >= half, 8 - half, 0))
        at = rank - me * half
        mine.append(jnp.where((at >= 0) & (at < half), name * half + at, -1))
    hit = functools.reduce(jnp.logical_or, [iota(pick.shape, 0) == b for b in back])
    pick[...] = jnp.where(hit, 1.0, 0.0).astype(BF16)
    row = iota((slots, tokens), 0)
    hits = [row == m for m in mine]
    scale[...] = sum(
        jnp.sum(jnp.where(h, weights[k : k + 1, :], 0.0), axis=1, keepdims=True)
        for k, h in enumerate(hits)
    )
    choose[...] = jnp.where(functools.reduce(jnp.logical_or, hits), 1.0, 0.0).astype(BF16)


def route_slots(core, routes, weights, experts, half):
    tokens, slots = routes.shape[1], experts * half
    out = (whole((experts * 16, tokens), BF16), whole((slots, tokens), BF16), whole((slots, 1), F32))
    body = functools.partial(route_body, experts=experts, half=half)
    return call(body, out, core, routes, weights, scalars=1, loose=(1, 2), kept=(1, 2))


def fill_body(core, choose, scale, mine, peer, send, rows):
    me = core[0]
    slots = choose.shape[0]
    for a in range(2):
        for n in range(2):
            for c in range(2):
                x = jnp.where(me == c, mine[n, a], peer[n, a])
                r = dot(choose[...], x, ((1,), (0,)))
                rows[pl.ds(4 * a + 2 * n + c, slots, stride=8), :] = scale[...] * r if a else r
    send[...] = rows[...].astype(BF16)


def fill_slots(core, choose, scale, mine, peer):
    fw = mine.shape[-1]
    total = choose.shape[0] * 8
    out = (whole((total, fw), BF16),)
    scratch = [pltpu.VMEM((total, fw), F32)]
    return call(fill_body, out, core, choose, scale, mine, peer, scalars=1, scratch=scratch, kept=(0,))


def sort_body(recv, both, near, rows):
    slots = recv.shape[0] // 8
    rows[...] = recv[...].astype(F32)
    for a in range(2):
        for n in range(2):
            for c in range(2):
                v = rows[pl.ds(4 * a + 2 * n + c, slots, stride=8), :].astype(BF16)
                both[n, 2 * a + c] = v
                if n == 0:
                    near[2 * a + c] = v


def sort_pieces(recv):
    slots, fw = recv.shape[0] // 8, recv.shape[1]
    out = (whole((2, 4, slots, fw), BF16), whole((4, slots, fw), BF16))
    return call(sort_body, out, recv, scratch=[pltpu.VMEM(recv.shape, F32)], kept=(0, 1))


def shards(chip, both, f1, b1, f2, b2, n_y):
    found = []
    for off, ref in ((0, both), (n_y - 1, f1), (1, b1)):
        for n in range(2):
            found.append((off + 4 * n, [ref[n, i] for i in range(4)]))
    for off, ref in ((n_y - 2, f2), (2, b2)):
        found.append((off, [ref[i] for i in range(4)]))
    for off, p in found:
        y = lax.rem(chip + off, n_y)
        yield y, jnp.concatenate(p[:2], axis=1), jnp.concatenate(p[2:], axis=1)


def expert_body(chip, both, f1, b1, f2, b2, wgu_peer, wg, wu, wd, wd_peer, gu_grad, hidden, part):
    n_y = part.shape[0]
    fw = wd.shape[0]
    rows, hid = hidden.shape
    acc = jnp.zeros((rows, 2 * hid), F32)
    back = jnp.zeros((rows, hid), F32)

    def weights(y):
        at = pl.ds(pl.multiple_of(y * 2 * fw, 2 * fw), 2 * fw)
        return jnp.concatenate([wg[at, :], wgu_peer[0, at, :], wu[at, :], wgu_peer[1, at, :]], axis=1), at

    for y, x_in, x_cot in shards(chip[0], both, f1, b1, f2, b2, n_y):
        w, at = weights(y)
        acc = acc + dot(x_in, w, ((1,), (0,)))
        back = back + dot(x_cot, jnp.concatenate([wd[:, at], wd_peer[:, at]], axis=0), ((1,), (1,)))
    gate, up = acc[:, :hid], acc[:, hid:]
    squash = jax.nn.sigmoid(gate)
    silu = gate * squash
    hidden[...] = (silu * up).astype(BF16)
    g_grad = (back * up * squash * (1.0 + gate * (1.0 - squash))).astype(BF16)
    u_grad = (back * silu).astype(BF16)
    grads = jnp.concatenate([g_grad, u_grad], axis=1)
    gu_grad[...] = grads
    for y in range(n_y):
        w, _ = weights(y)
        r = dot(grads, w, ((1,), (1,))).astype(BF16)
        part[y, 0] = r[:, :fw]
        part[y, 1] = r[:, fw:]


def expert_rows_grad(chip, blocks, wgu_peer, wg, wu, wd, wd_peer, n_y):
    rows, fw = blocks[0].shape[2:]
    hid = 2 * wg.shape[1]

    out = (whole((rows, 2 * hid), BF16), whole((rows, hid), BF16), whole((n_y, 2, rows, fw), BF16))
    weights = (wgu_peer, wg, wu, wd, wd_peer)
    return call(expert_body, out, chip, *blocks, *weights, scalars=1)


def weight_body(chip, both, f1, b1, f2, b2, gu_grad, hidden, dgu, dgu_send, dd, dd_send):
    fw = dd.shape[0]
    hid = hidden.shape[1]
    n_y = dd.shape[1] // (2 * fw)
    for y, x_in, x_cot in shards(chip[0], both, f1, b1, f2, b2, n_y):
        at = pl.ds(pl.multiple_of(y * 2 * fw, 2 * fw), 2 * fw)
        r = dot(x_in, gu_grad[...], ((0,), (0,))).astype(BF16)
        for i in range(2):
            dgu[i, at, :] = r[:, i * hid : i * hid + fw]
            dgu_send[i, at, :] = r[:, i * hid + fw : (i + 1) * hid]
        r = dot(hidden[...], x_cot, ((0,), (0,))).astype(BF16)
        dd[:, at] = r[:fw]
        dd_send[:, at] = r[fw:]


def expert_weight_grads(chip, blocks, gu_grad, hidden, d):
    fw = blocks[0].shape[3]
    out = (whole((2, d, fw), BF16),) * 2 + (whole((fw, d), BF16),) * 2
    return call(weight_body, out, chip, *blocks, gu_grad, hidden, scalars=1, loose=(6, 7))


def add_body(parts, out, *, half):
    n_y, n_h, rows, _ = parts.shape
    j, r = iota((out.shape[0], rows), 0), iota((out.shape[0], rows), 1)
    slot = j & 7
    source = (j >> 4) * half + slot
    total = 0.0
    for h in range(n_h):
        s = parts[0, h].astype(F32)
        for y in range(1, n_y):
            s = s + parts[y, h].astype(F32)
        hit = (source == r) & (slot < half) & (((j >> 3) & 1) == h)
        total = total + dot(jnp.where(hit, 1.0, 0.0).astype(BF16), s.astype(BF16), ((1,), (0,)))
    out[...] = total.astype(BF16)


def add_parts(parts, blocks, half):
    out = (whole((blocks * 16, parts.shape[3]), BF16),)
    return call(functools.partial(add_body, half=half), out, parts, kept=(0,))


def later(v, step, fill):
    return jnp.concatenate([v[step:], jnp.full((step, v.shape[1]), fill, v.dtype)], axis=0)


def in_three(v):
    hi = v.astype(BF16)
    mid = (v - hi.astype(F32)).astype(BF16)
    lo = (v - hi.astype(F32) - mid.astype(F32)).astype(BF16)
    return [p.astype(F32) for p in (hi, mid, lo)]


def chain_body(mix, out_proj, rec_state, decay, local, through, last):
    n_sp, width = last.shape[0], last.shape[2]
    keep = mix.shape[1] // n_sp
    proj = dot(mix[...], rec_state[...], ((0,), (0,))).astype(BF16)
    for k in range(n_sp):
        last[k, :keep, :] = proj[k * keep : (k + 1) * keep, :]
    grad = dot(mix[...], out_proj[...], ((1,), (1,)))
    mult = later(decay[...], 1, 1.0)
    step = 1
    while step < grad.shape[0]:
        grad = grad + mult * later(grad, step, 0.0)
        mult = mult * later(mult, step, 1.0)
        step *= 2
    local[...] = grad
    through[...] = mult
    first = decay[0:1, :]
    row = iota((last.shape[1] - keep, width), 0)
    chain = jnp.zeros(row.shape, F32)
    for i, piece in enumerate(in_three(first * mult[0:1, :]) + in_three(first * grad[0:1, :])):
        chain = jnp.where(row == i, piece, chain)
    chain = chain.astype(BF16)
    for k in range(n_sp):
        last[k, keep:, :] = chain


def chain_within(mix, out_proj, rec_state, decay, n_sp):
    tokens, width = decay.shape
    last = whole((n_sp, mix.shape[1] // n_sp + 8, width), BF16)
    out = (whole((tokens, width), F32),) * 2 + (last,)
    return call(chain_body, out, mix, out_proj, rec_state, decay, kept=(0, 1, 2))


def finish_body(here, last, local, through, value_by, input_by, rate_by, proj, value, inp, rate):
    n_sp = last.shape[0]
    keep = proj.shape[0]
    incoming = jnp.zeros((1, last.shape[2]), F32)
    for k in reversed(range(n_sp)):
        c = last[k, keep:, :].astype(F32)
        mult = (c[2:3] + c[1:2]) + c[0:1]
        add = (c[5:6] + c[4:5]) + c[3:4]
        incoming = jnp.where(k > here[0], add + mult * incoming, incoming)
    carried = local[...] + through[...] * incoming
    value[...] = (carried * value_by[...]).astype(BF16)
    inp[...] = (carried * input_by[...]).astype(BF16)
    rate[...] = (carried * rate_by[...]).astype(BF16)
    total = last[0, :keep, :].astype(F32)
    for k in range(1, n_sp):
        total = total + last[k, :keep, :].astype(F32)
    proj[...] = total


def finish(here, last, local, through, value_by, input_by, rate_by):
    grid = whole(local.shape, BF16)
    out = (whole((last.shape[1] - 8, last.shape[2]), F32), grid, grid, grid)
    return call(finish_body, out, here, last, local, through, value_by, input_by, rate_by, scalars=1)


def per_device(
    ffn_input,
    out_grad,
    routes,
    route_weight,
    gate_w,
    up_w,
    down_w,
    out_proj,
    rec_value,
    rate_pre,
    input_pre,
    prev_state,
    decay_param,
):
    n_sp, n_y = lax.axis_size(SP), lax.axis_size("y")
    tok, count = routes.shape
    half = 5 * count * tok // (8 * n_sp)
    fw = ffn_input.shape[1]
    d = gate_w.shape[1]
    chip = lax.axis_index("y").reshape(1).astype(jnp.int32)
    core = lax.axis_index("c").reshape(1).astype(jnp.int32)

    def over_y(v, step):
        return lax.ppermute(v, "y", [(i, (i + step) % n_y) for i in range(n_y)])

    def over_cores(v):
        return lax.ppermute(v, "c", [(0, 1), (1, 0)])

    own = jnp.stack([ffn_input, out_grad])
    far = over_y(own, n_y // 2)
    mine = jnp.stack([own, far])
    peer = over_cores(mine)
    pick, choose, scale = route_slots(core, routes.T, route_weight.T, n_sp, half)
    send = fill_slots(core, choose, scale, mine, peer)

    recv = lax.all_to_all(send.reshape(n_sp, -1, fw), SP, 0, 0, tiled=True).reshape(send.shape)
    both, near = sort_pieces(recv)

    near, late_gate, late_up, late_down = lax.optimization_barrier((near, gate_w, up_w, down_w))
    wgu = jnp.concatenate([late_gate, late_up], axis=0)
    wgu_peer = over_cores(wgu)
    wd_peer = over_cores(late_down[0])
    first = (both, over_y(both, 1), over_y(both, -1))
    blocks = (*first, over_y(near, 2), over_y(near, -2))

    gu_grad, hidden, part = expert_rows_grad(
        chip, blocks, wgu_peer, late_gate[0], late_up[0], late_down[0], wd_peer, n_y
    )
    rate_gate = jax.nn.sigmoid(rate_pre.astype(F32))
    input_gate = jax.nn.sigmoid(input_pre.astype(F32))
    decay_speed = jax.nn.softplus(-decay_param)[None, :]
    log_decay = -decay_scale * rate_gate * decay_speed
    decay = jnp.exp(log_decay)
    scale_in = jnp.sqrt(-jnp.expm1(2.0 * log_decay))
    signal = rec_value.astype(F32)
    before_state = prev_state.astype(F32)
    rec_state = (decay * before_state + scale_in * input_gate * signal).astype(BF16)
    value_by = scale_in * input_gate
    input_by = value_by * signal * (1.0 - input_gate)
    decay_part = decay * before_state - input_gate * signal * decay * decay / scale_in
    rate_by = decay_part * (-decay_scale * decay_speed) * rate_gate * (1.0 - rate_gate)
    here = lax.axis_index(SP).reshape(1).astype(jnp.int32)
    part, here = lax.optimization_barrier((part, here))
    arrived = lax.all_to_all(part.reshape(2 * n_y, *part.shape[2:]), TP, 0, 0, tiled=True)
    back = add_parts(arrived.reshape(part.shape), n_sp, half)
    returned = lax.all_to_all(back.reshape(n_sp, 16, fw), SP, 0, 0, tiled=True).reshape(back.shape)
    dgu, dgu_send, dd, dd_send = expert_weight_grads(chip, blocks, gu_grad, hidden, d)
    dgu_peer = over_cores(dgu_send)
    dd_peer = over_cores(dd_send)
    d_gate, d_up = [(dgu[i].astype(F32) + dgu_peer[i].astype(F32)).astype(BF16)[None] for i in range(2)]
    d_down = (dd.astype(F32) + dd_peer.astype(F32)).astype(BF16)[None]
    own_grad = (dot(pick, returned, ((0,), (0,))) + out_grad.astype(F32)).astype(BF16)
    mix_grad = lax.all_gather(own_grad, TP, axis=1, tiled=True)

    local, through, last = chain_within(mix_grad, out_proj, rec_state, decay, n_sp)
    last = lax.all_to_all(last, SP, 0, 0, tiled=True)
    out_proj_grad, rec_value_grad, input_pre_grad, rate_pre_grad = finish(
        here, last, local, through, value_by, input_by, rate_by
    )
    return (
        d_gate,
        d_up,
        d_down,
        out_proj_grad,
        rec_value_grad,
        rate_pre_grad,
        input_pre_grad,
    )


def solution(mesh):
    finer = Mesh(mesh.devices.reshape(8, 4, 8, 2), ("z", "x", "y", "c"))
    grid = P(SP, TP)
    return jax.shard_map(
        per_device,
        mesh=finer,
        in_specs=(
            grid,
            grid,
            P(SP, None),
            P(SP, None),
            P(SP, None, TP),
            P(SP, None, TP),
            P(SP, TP, None),
            P(TP, None),
            grid,
            grid,
            grid,
            grid,
            P(TP),
        ),
        out_specs=(P(SP, None, TP), P(SP, None, TP), P(SP, TP, None), grid, grid, grid, grid),
        check_vma=False,
    )
```

```python
import functools

import jax
import jax.numpy as jnp
from jax import lax
from jax.experimental import pallas as pl
from jax.experimental.pallas import tpu as pltpu
from jax.sharding import Mesh
from jax.sharding import PartitionSpec as P

SP = ("z", "x")
TP = ("y", "c")
F32 = jnp.float32
BF16 = jnp.bfloat16
decay_scale = 8.0

SMEM = pl.BlockSpec(memory_space=pltpu.SMEM)
VMEM = pl.BlockSpec(memory_space=pltpu.VMEM)


def whole(shape, dtype):
    return jax.ShapeDtypeStruct(shape, dtype)


def call(body, out, *operands, scalars=0, scratch=(), loose=(), kept=()):
    held = [
        o if i < scalars or i in loose else pltpu.with_memory_space_constraint(o, pltpu.VMEM)
        for i, o in enumerate(operands)
    ]
    outs = [(pltpu.VMEM if i in kept else pltpu.HBM)(o.shape, o.dtype) for i, o in enumerate(out)]
    got = pl.pallas_call(
        body,
        out_shape=tuple(outs),
        in_specs=[SMEM] * scalars + [VMEM] * (len(operands) - scalars),
        out_specs=tuple([VMEM] * len(outs)),
        scratch_shapes=list(scratch),
        compiler_params=pltpu.CompilerParams(vmem_limit_bytes=16 * 2**20),
    )(*held)
    return got if len(out) > 1 else got[0]


def dot(a, b, dims):
    return lax.dot_general(a, b, (dims, ((), ())), preferred_element_type=F32)


def iota(shape, dim):
    return lax.broadcasted_iota(jnp.int32, shape, dim)


def route_body(core, routes, weights, pick, choose, scale, *, experts, half):
    me = core[0]
    count, tokens = routes.shape
    slots = experts * half
    here = [iota((experts, tokens), 0) == routes[k : k + 1, :] for k in range(count)]
    named = functools.reduce(jnp.logical_or, here)
    earlier = iota((tokens, tokens), 0) < iota((tokens, tokens), 1)
    before = dot(
        jnp.where(named, 1.0, 0.0).astype(BF16), jnp.where(earlier, 1.0, 0.0).astype(BF16), ((1,), (0,))
    )
    back, mine = [], []
    for k in range(count):
        rank = jnp.sum(jnp.where(here[k], before, 0.0), axis=0, keepdims=True).astype(jnp.int32)
        name = routes[k : k + 1, :]
        back.append(name * 16 + rank + jnp.where(rank >= half, 8 - half, 0))
        at = rank - me * half
        mine.append(jnp.where((at >= 0) & (at < half), name * half + at, -1))
    hit = functools.reduce(jnp.logical_or, [iota(pick.shape, 0) == b for b in back])
    pick[...] = jnp.where(hit, 1.0, 0.0).astype(BF16)
    row = iota((slots, tokens), 0)
    hits = [row == m for m in mine]
    scale[...] = sum(
        jnp.sum(jnp.where(h, weights[k : k + 1, :], 0.0), axis=1, keepdims=True)
        for k, h in enumerate(hits)
    )
    choose[...] = jnp.where(functools.reduce(jnp.logical_or, hits), 1.0, 0.0).astype(BF16)


def route_slots(core, routes, weights, experts, half):
    tokens, slots = routes.shape[1], experts * half
    out = (whole((experts * 16, tokens), BF16), whole((slots, tokens), BF16), whole((slots, 1), F32))
    body = functools.partial(route_body, experts=experts, half=half)
    return call(body, out, core, routes, weights, scalars=1, loose=(1, 2), kept=(1, 2))


def fill_body(core, choose, scale, mine, peer, send, rows):
    me = core[0]
    slots = choose.shape[0]
    for a in range(2):
        for n in range(2):
            for c in range(2):
                x = jnp.where(me == c, mine[n, a], peer[n, a])
                r = dot(choose[...], x, ((1,), (0,)))
                rows[pl.ds(4 * a + 2 * n + c, slots, stride=8), :] = scale[...] * r if a else r
    send[...] = rows[...].astype(BF16)


def fill_slots(core, choose, scale, mine, peer):
    fw = mine.shape[-1]
    total = choose.shape[0] * 8
    out = (whole((total, fw), BF16),)
    scratch = [pltpu.VMEM((total, fw), F32)]
    return call(fill_body, out, core, choose, scale, mine, peer, scalars=1, scratch=scratch, kept=(0,))


def sort_body(recv, both, near, rows):
    slots = recv.shape[0] // 8
    rows[...] = recv[...].astype(F32)
    for a in range(2):
        for n in range(2):
            for c in range(2):
                v = rows[pl.ds(4 * a + 2 * n + c, slots, stride=8), :].astype(BF16)
                both[n, 2 * a + c] = v
                if n == 0:
                    near[2 * a + c] = v


def sort_pieces(recv):
    slots, fw = recv.shape[0] // 8, recv.shape[1]
    out = (whole((2, 4, slots, fw), BF16), whole((4, slots, fw), BF16))
    return call(sort_body, out, recv, scratch=[pltpu.VMEM(recv.shape, F32)], kept=(0, 1))


def shards(chip, both, f1, b1, f2, b2, near, n_y):
    found = []
    for off, ref in ((0, both), (n_y - 1, f1), (1, b1)):
        for n in range(2):
            found.append((off + 4 * n, [near[i] if off == n == 0 else ref[n, i] for i in range(4)]))
    for off, ref in ((n_y - 2, f2), (2, b2)):
        found.append((off, [ref[i] for i in range(4)]))
    for off, p in found:
        y = lax.rem(chip + off, n_y)
        yield y, jnp.concatenate(p[:2], axis=1), jnp.concatenate(p[2:], axis=1)


def expert_body(chip, both, f1, b1, f2, b2, near, wgu_peer, wg, wu, wd, wd_peer, gu_grad, hidden, part):
    n_y = part.shape[0]
    fw = wd.shape[0]
    rows, hid = hidden.shape
    acc = jnp.zeros((rows, 2 * hid), F32)
    back = jnp.zeros((rows, hid), F32)

    def weights(y):
        at = pl.ds(pl.multiple_of(y * 2 * fw, 2 * fw), 2 * fw)
        return jnp.concatenate([wg[at, :], wgu_peer[0, at, :], wu[at, :], wgu_peer[1, at, :]], axis=1), at

    for y, x_in, x_cot in shards(chip[0], both, f1, b1, f2, b2, near, n_y):
        w, at = weights(y)
        acc = acc + dot(x_in, w, ((1,), (0,)))
        back = back + dot(x_cot, jnp.concatenate([wd[:, at], wd_peer[:, at]], axis=0), ((1,), (1,)))
    gate, up = acc[:, :hid], acc[:, hid:]
    squash = jax.nn.sigmoid(gate)
    silu = gate * squash
    hidden[...] = (silu * up).astype(BF16)
    g_grad = (back * up * squash * (1.0 + gate * (1.0 - squash))).astype(BF16)
    u_grad = (back * silu).astype(BF16)
    grads = jnp.concatenate([g_grad, u_grad], axis=1)
    gu_grad[...] = grads
    for y in range(n_y):
        w, _ = weights(y)
        r = dot(grads, w, ((1,), (1,))).astype(BF16)
        part[y, 0] = r[:, :fw]
        part[y, 1] = r[:, fw:]


def expert_rows_grad(chip, blocks, wgu_peer, wg, wu, wd, wd_peer, n_y):
    rows, fw = blocks[0].shape[2:]
    hid = 2 * wg.shape[1]

    out = (whole((rows, 2 * hid), BF16), whole((rows, hid), BF16), whole((n_y, 2, rows, fw), BF16))
    weights = (wgu_peer, wg, wu, wd, wd_peer)
    return call(expert_body, out, chip, *blocks, *weights, scalars=1)


def weight_body(chip, both, f1, b1, f2, b2, near, gu_grad, hidden, dgu, dgu_send, dd, dd_send):
    fw = dd.shape[0]
    hid = hidden.shape[1]
    n_y = dd.shape[1] // (2 * fw)
    for y, x_in, x_cot in shards(chip[0], both, f1, b1, f2, b2, near, n_y):
        at = pl.ds(pl.multiple_of(y * 2 * fw, 2 * fw), 2 * fw)
        r = dot(x_in, gu_grad[...], ((0,), (0,))).astype(BF16)
        for i in range(2):
            dgu[i, at, :] = r[:, i * hid : i * hid + fw]
            dgu_send[i, at, :] = r[:, i * hid + fw : (i + 1) * hid]
        r = dot(hidden[...], x_cot, ((0,), (0,))).astype(BF16)
        dd[:, at] = r[:fw]
        dd_send[:, at] = r[fw:]


def expert_weight_grads(chip, blocks, gu_grad, hidden, d):
    fw = blocks[0].shape[3]
    out = (whole((2, d, fw), BF16),) * 2 + (whole((fw, d), BF16),) * 2
    return call(weight_body, out, chip, *blocks, gu_grad, hidden, scalars=1, loose=(7, 8))


def add_body(parts, out, *, half):
    n_y, n_h, rows, _ = parts.shape
    j, r = iota((out.shape[0], rows), 0), iota((out.shape[0], rows), 1)
    slot = j & 7
    source = (j >> 4) * half + slot
    total = 0.0
    for h in range(n_h):
        s = parts[0, h].astype(F32)
        for y in range(1, n_y):
            s = s + parts[y, h].astype(F32)
        hit = (source == r) & (slot < half) & (((j >> 3) & 1) == h)
        total = total + dot(jnp.where(hit, 1.0, 0.0).astype(BF16), s.astype(BF16), ((1,), (0,)))
    out[...] = total.astype(BF16)


def add_parts(parts, blocks, half):
    out = (whole((blocks * 16, parts.shape[3]), BF16),)
    return call(functools.partial(add_body, half=half), out, parts, kept=(0,))


def later(v, step, fill):
    return jnp.concatenate([v[step:], jnp.full((step, v.shape[1]), fill, v.dtype)], axis=0)


def in_three(v):
    hi = v.astype(BF16)
    mid = (v - hi.astype(F32)).astype(BF16)
    lo = (v - hi.astype(F32) - mid.astype(F32)).astype(BF16)
    return [p.astype(F32) for p in (hi, mid, lo)]


def chain_rows(mult, add, shape):
    row = iota(shape, 0)
    chain = jnp.zeros(shape, F32)
    for i, piece in enumerate(in_three(mult) + in_three(add)):
        chain = jnp.where(row == i, piece, chain)
    return chain.astype(BF16)


def chain_of(rows):
    c = rows.astype(F32)
    return (c[2:3] + c[1:2]) + c[0:1], (c[5:6] + c[4:5]) + c[3:4]


def chain_body(mix, out_proj, rec_state, decay, local, through, last):
    n_x, n_z, _, width = last.shape
    keep = mix.shape[1] // (n_x * n_z)
    proj = dot(mix[...], rec_state[...], ((0,), (0,))).astype(BF16)
    for k in range(n_x * n_z):
        last[k % n_x, k // n_x, :keep, :] = proj[k * keep : (k + 1) * keep, :]
    grad = dot(mix[...], out_proj[...], ((1,), (1,)))
    mult = later(decay[...], 1, 1.0)
    step = 1
    while step < grad.shape[0]:
        grad = grad + mult * later(grad, step, 0.0)
        mult = mult * later(mult, step, 1.0)
        step *= 2
    local[...] = grad
    through[...] = mult
    first = decay[0:1, :]
    chain = chain_rows(first * mult[0:1, :], first * grad[0:1, :], (last.shape[2] - keep, width))
    for k in range(n_x * n_z):
        last[k % n_x, k // n_x, keep:, :] = chain


def chain_within(mix, out_proj, rec_state, decay, n_x, n_z):
    tokens, width = decay.shape
    last = whole((n_x, n_z, mix.shape[1] // (n_x * n_z) + 8, width), BF16)
    out = (whole((tokens, width), F32),) * 2 + (last,)
    return call(chain_body, out, mix, out_proj, rec_state, decay, kept=(0, 1, 2))


def join_body(here, last, sent, within):
    n_x, n_z, rows, width = last.shape
    keep = rows - 8
    for z in range(n_z):
        total = last[0, z, :keep, :].astype(F32)
        for x in range(1, n_x):
            total = total + last[x, z, :keep, :].astype(F32)
        sent[z, :keep, :] = total.astype(BF16)
    mult, add = jnp.ones((1, width), F32), jnp.zeros((1, width), F32)
    after = [mult, add]
    for x in reversed(range(n_x)):
        m, a = chain_of(last[x, 0, keep:, :])
        passed = x > here[0]
        after = [jnp.where(passed, m * after[0], after[0]), jnp.where(passed, a + m * after[1], after[1])]
        mult, add = m * mult, a + m * add
    row = iota(within.shape, 0)
    within[...] = jnp.where(row == 0, after[0], after[1])
    chain = chain_rows(mult, add, (8, width))
    for z in range(n_z):
        sent[z, keep:, :] = chain


def join(here, last):
    out = (whole(last.shape[1:], BF16), whole((8, last.shape[3]), F32))
    return call(join_body, out, here, last, scalars=1, kept=(0, 1))


def finish_body(here, last, within, local, through, value_by, input_by, rate_by, proj, value, inp, rate):
    n_z = last.shape[0]
    keep = proj.shape[0]
    incoming = jnp.zeros((1, last.shape[2]), F32)
    for k in reversed(range(n_z)):
        mult, add = chain_of(last[k, keep:, :])
        incoming = jnp.where(k > here[0], add + mult * incoming, incoming)
    incoming = within[1:2, :] + within[0:1, :] * incoming
    carried = local[...] + through[...] * incoming
    value[...] = (carried * value_by[...]).astype(BF16)
    inp[...] = (carried * input_by[...]).astype(BF16)
    rate[...] = (carried * rate_by[...]).astype(BF16)
    total = last[0, :keep, :].astype(F32)
    for k in range(1, n_z):
        total = total + last[k, :keep, :].astype(F32)
    proj[...] = total


def finish(here, last, within, local, through, value_by, input_by, rate_by):
    grid = whole(local.shape, BF16)
    out = (whole((last.shape[1] - 8, last.shape[2]), F32), grid, grid, grid)
    return call(finish_body, out, here, last, within, local, through, value_by, input_by, rate_by, scalars=1)


def per_device(
    ffn_input,
    out_grad,
    routes,
    route_weight,
    gate_w,
    up_w,
    down_w,
    out_proj,
    rec_value,
    rate_pre,
    input_pre,
    prev_state,
    decay_param,
):
    n_sp, n_y = lax.axis_size(SP), lax.axis_size("y")
    tok, count = routes.shape
    half = 5 * count * tok // (8 * n_sp)
    fw = ffn_input.shape[1]
    d = gate_w.shape[1]
    chip = lax.axis_index("y").reshape(1).astype(jnp.int32)
    core = lax.axis_index("c").reshape(1).astype(jnp.int32)

    def over_y(v, step):
        return lax.ppermute(v, "y", [(i, (i + step) % n_y) for i in range(n_y)])

    def over_cores(v):
        return lax.ppermute(v, "c", [(0, 1), (1, 0)])

    own = jnp.stack([ffn_input, out_grad])
    far = over_y(own, n_y // 2)
    mine = jnp.stack([own, far])
    peer = over_cores(mine)
    pick, choose, scale = route_slots(core, routes.T, route_weight.T, n_sp, half)
    send = fill_slots(core, choose, scale, mine, peer)

    recv = lax.all_to_all(send.reshape(n_sp, -1, fw), SP, 0, 0, tiled=True).reshape(send.shape)
    both, near = sort_pieces(recv)

    near, late_gate, late_up, late_down = lax.optimization_barrier((near, gate_w, up_w, down_w))
    wgu = jnp.concatenate([late_gate, late_up], axis=0)
    wgu_peer = over_cores(wgu)
    wd_peer = over_cores(late_down[0])
    first = (both, over_y(both, 1), over_y(both, -1))
    blocks = (*first, over_y(near, 2), over_y(near, -2), near)

    gu_grad, hidden, part = expert_rows_grad(
        chip, blocks, wgu_peer, late_gate[0], late_up[0], late_down[0], wd_peer, n_y
    )
    rate_gate = jax.nn.sigmoid(rate_pre.astype(F32))
    input_gate = jax.nn.sigmoid(input_pre.astype(F32))
    decay_speed = jax.nn.softplus(-decay_param)[None, :]
    log_decay = -decay_scale * rate_gate * decay_speed
    decay = jnp.exp(log_decay)
    scale_in = jnp.sqrt(-jnp.expm1(2.0 * log_decay))
    signal = rec_value.astype(F32)
    before_state = prev_state.astype(F32)
    rec_state = (decay * before_state + scale_in * input_gate * signal).astype(BF16)
    value_by = scale_in * input_gate
    input_by = value_by * signal * (1.0 - input_gate)
    decay_part = decay * before_state - input_gate * signal * decay * decay / scale_in
    rate_by = decay_part * (-decay_scale * decay_speed) * rate_gate * (1.0 - rate_gate)
    my_z = lax.axis_index("z").reshape(1).astype(jnp.int32)
    my_x = lax.axis_index("x").reshape(1).astype(jnp.int32)
    part, my_z, my_x = lax.optimization_barrier((part, my_z, my_x))
    arrived = lax.all_to_all(part.reshape(2 * n_y, *part.shape[2:]), TP, 0, 0, tiled=True)
    back = add_parts(arrived.reshape(part.shape), n_sp, half)
    returned = lax.all_to_all(back.reshape(n_sp, 16, fw), SP, 0, 0, tiled=True).reshape(back.shape)
    dgu, dgu_send, dd, dd_send = expert_weight_grads(chip, blocks, gu_grad, hidden, d)
    dgu_peer = over_cores(dgu_send)
    dd_peer = over_cores(dd_send)
    d_gate, d_up = [(dgu[i].astype(F32) + dgu_peer[i].astype(F32)).astype(BF16)[None] for i in range(2)]
    d_down = (dd.astype(F32) + dd_peer.astype(F32)).astype(BF16)[None]
    own_grad = (dot(pick, returned, ((0,), (0,))) + out_grad.astype(F32)).astype(BF16)
    mix_grad = lax.all_gather(own_grad, TP, axis=1, tiled=True)

    n_x, n_z = lax.axis_size("x"), lax.axis_size("z")
    local, through, last = chain_within(mix_grad, out_proj, rec_state, decay, n_x, n_z)
    over_x = lax.all_to_all(last.reshape(n_x, -1, fw), "x", 0, 0, tiled=True)
    sent, within = join(my_x, over_x.reshape(last.shape))
    last = lax.all_to_all(sent, "z", 0, 0, tiled=True)
    out_proj_grad, rec_value_grad, input_pre_grad, rate_pre_grad = finish(
        my_z, last, within, local, through, value_by, input_by, rate_by
    )
    return (
        d_gate,
        d_up,
        d_down,
        out_proj_grad,
        rec_value_grad,
        rate_pre_grad,
        input_pre_grad,
    )


def solution(mesh):
    finer = Mesh(mesh.devices.reshape(8, 4, 8, 2), ("z", "x", "y", "c"))
    grid = P(SP, TP)
    return jax.shard_map(
        per_device,
        mesh=finer,
        in_specs=(
            grid,
            grid,
            P(SP, None),
            P(SP, None),
            P(SP, None, TP),
            P(SP, None, TP),
            P(SP, TP, None),
            P(TP, None),
            grid,
            grid,
            grid,
            grid,
            P(TP),
        ),
        out_specs=(P(SP, None, TP), P(SP, None, TP), P(SP, TP, None), grid, grid, grid, grid),
        check_vma=False,
    )
```

```python
import functools

import jax
import jax.numpy as jnp
from jax import lax
from jax.experimental import pallas as pl
from jax.experimental.pallas import tpu as pltpu
from jax.sharding import Mesh
from jax.sharding import PartitionSpec as P

SP = ("z", "x")
TP = ("y", "c")
F32 = jnp.float32
BF16 = jnp.bfloat16
decay_scale = 8.0

SMEM = pl.BlockSpec(memory_space=pltpu.SMEM)
VMEM = pl.BlockSpec(memory_space=pltpu.VMEM)


def whole(shape, dtype):
    return jax.ShapeDtypeStruct(shape, dtype)


def call(body, out, *operands, scalars=0, scratch=(), loose=(), kept=()):
    held = [
        o if i < scalars or i in loose else pltpu.with_memory_space_constraint(o, pltpu.VMEM)
        for i, o in enumerate(operands)
    ]
    outs = [(pltpu.VMEM if i in kept else pltpu.HBM)(o.shape, o.dtype) for i, o in enumerate(out)]
    got = pl.pallas_call(
        body,
        out_shape=tuple(outs),
        in_specs=[SMEM] * scalars + [VMEM] * (len(operands) - scalars),
        out_specs=tuple([VMEM] * len(outs)),
        scratch_shapes=list(scratch),
        compiler_params=pltpu.CompilerParams(vmem_limit_bytes=16 * 2**20),
    )(*held)
    return got if len(out) > 1 else got[0]


def dot(a, b, dims):
    return lax.dot_general(a, b, (dims, ((), ())), preferred_element_type=F32)


def iota(shape, dim):
    return lax.broadcasted_iota(jnp.int32, shape, dim)


def route_body(core, routes, weights, pick, choose, scale, *, experts, half):
    me = core[0]
    count, tokens = routes.shape
    slots = experts * half
    here = [iota((experts, tokens), 0) == routes[k : k + 1, :] for k in range(count)]
    named = functools.reduce(jnp.logical_or, here)
    earlier = iota((tokens, tokens), 0) < iota((tokens, tokens), 1)
    before = dot(
        jnp.where(named, 1.0, 0.0).astype(BF16), jnp.where(earlier, 1.0, 0.0).astype(BF16), ((1,), (0,))
    )
    back, mine = [], []
    for k in range(count):
        rank = jnp.sum(jnp.where(here[k], before, 0.0), axis=0, keepdims=True).astype(jnp.int32)
        name = routes[k : k + 1, :]
        back.append(name * 16 + rank + jnp.where(rank >= half, 8 - half, 0))
        at = rank - me * half
        mine.append(jnp.where((at >= 0) & (at < half), name * half + at, -1))
    hit = functools.reduce(jnp.logical_or, [iota(pick.shape, 0) == b for b in back])
    pick[...] = jnp.where(hit, 1.0, 0.0).astype(BF16)
    row = iota((slots, tokens), 0)
    hits = [row == m for m in mine]
    scale[...] = sum(
        jnp.sum(jnp.where(h, weights[k : k + 1, :], 0.0), axis=1, keepdims=True)
        for k, h in enumerate(hits)
    )
    choose[...] = jnp.where(functools.reduce(jnp.logical_or, hits), 1.0, 0.0).astype(BF16)


def route_slots(core, routes, weights, experts, half):
    tokens, slots = routes.shape[1], experts * half
    out = (whole((experts * 16, tokens), BF16), whole((slots, tokens), BF16), whole((slots, 1), F32))
    body = functools.partial(route_body, experts=experts, half=half)
    return call(body, out, core, routes, weights, scalars=1, loose=(1, 2), kept=(1, 2))


def fill_body(core, choose, scale, mine, peer, send, rows):
    me = core[0]
    slots = choose.shape[0]
    for a in range(2):
        for n in range(2):
            for c in range(2):
                x = jnp.where(me == c, mine[n, a], peer[n, a])
                r = dot(choose[...], x, ((1,), (0,)))
                rows[pl.ds(4 * a + 2 * n + c, slots, stride=8), :] = scale[...] * r if a else r
    send[...] = rows[...].astype(BF16)


def fill_slots(core, choose, scale, mine, peer):
    fw = mine.shape[-1]
    total = choose.shape[0] * 8
    out = (whole((total, fw), BF16),)
    scratch = [pltpu.VMEM((total, fw), F32)]
    return call(fill_body, out, core, choose, scale, mine, peer, scalars=1, scratch=scratch, kept=(0,))


def sort_body(recv, both, near, rows):
    slots = recv.shape[0] // 8
    rows[...] = recv[...].astype(F32)
    for a in range(2):
        for n in range(2):
            for c in range(2):
                v = rows[pl.ds(4 * a + 2 * n + c, slots, stride=8), :].astype(BF16)
                both[n, 2 * a + c] = v
                if n == 0:
                    near[2 * a + c] = v


def sort_pieces(recv):
    slots, fw = recv.shape[0] // 8, recv.shape[1]
    out = (whole((2, 4, slots, fw), BF16), whole((4, slots, fw), BF16))
    return call(sort_body, out, recv, scratch=[pltpu.VMEM(recv.shape, F32)], kept=(0, 1))


def shards(chip, both, f1, b1, f2, b2, near, n_y):
    found = []
    for off, ref in ((0, both), (n_y - 1, f1), (1, b1)):
        for n in range(2):
            found.append((off + 4 * n, [near[i] if off == n == 0 else ref[n, i] for i in range(4)]))
    for off, ref in ((n_y - 2, f2), (2, b2)):
        found.append((off, [ref[i] for i in range(4)]))
    for off, p in found:
        y = lax.rem(chip + off, n_y)
        yield y, jnp.concatenate(p[:2], axis=1), jnp.concatenate(p[2:], axis=1)


def expert_body(chip, both, f1, b1, f2, b2, near, wgu_peer, wg, wu, wd, wd_peer, gu_grad, hidden, part):
    n_y = part.shape[0]
    fw = wd.shape[0]
    rows, hid = hidden.shape
    acc = jnp.zeros((rows, 2 * hid), F32)
    back = jnp.zeros((rows, hid), F32)

    def weights(y):
        at = pl.ds(pl.multiple_of(y * 2 * fw, 2 * fw), 2 * fw)
        return jnp.concatenate([wg[at, :], wgu_peer[0, at, :], wu[at, :], wgu_peer[1, at, :]], axis=1), at

    for y, x_in, x_cot in shards(chip[0], both, f1, b1, f2, b2, near, n_y):
        w, at = weights(y)
        acc = acc + dot(x_in, w, ((1,), (0,)))
        back = back + dot(x_cot, jnp.concatenate([wd[:, at], wd_peer[:, at]], axis=0), ((1,), (1,)))
    gate, up = acc[:, :hid], acc[:, hid:]
    squash = jax.nn.sigmoid(gate)
    silu = gate * squash
    hidden[...] = (silu * up).astype(BF16)
    g_grad = (back * up * squash * (1.0 + gate * (1.0 - squash))).astype(BF16)
    u_grad = (back * silu).astype(BF16)
    grads = jnp.concatenate([g_grad, u_grad], axis=1)
    gu_grad[...] = grads
    for y in range(n_y):
        w, _ = weights(y)
        r = dot(grads, w, ((1,), (1,))).astype(BF16)
        part[y, 0] = r[:, :fw]
        part[y, 1] = r[:, fw:]


def expert_rows_grad(chip, blocks, wgu_peer, wg, wu, wd, wd_peer, n_y):
    rows, fw = blocks[0].shape[2:]
    hid = 2 * wg.shape[1]

    out = (whole((rows, 2 * hid), BF16), whole((rows, hid), BF16), whole((n_y, 2, rows, fw), BF16))
    weights = (wgu_peer, wg, wu, wd, wd_peer)
    return call(expert_body, out, chip, *blocks, *weights, scalars=1)


def weight_body(chip, both, f1, b1, f2, b2, near, gu_grad, hidden, dgu, dgu_send, dd, dd_send):
    fw = dd.shape[0]
    hid = hidden.shape[1]
    n_y = dd.shape[1] // (2 * fw)
    for y, x_in, x_cot in shards(chip[0], both, f1, b1, f2, b2, near, n_y):
        at = pl.ds(pl.multiple_of(y * 2 * fw, 2 * fw), 2 * fw)
        r = dot(x_in, gu_grad[...], ((0,), (0,))).astype(BF16)
        for i in range(2):
            dgu[i, at, :] = r[:, i * hid : i * hid + fw]
            dgu_send[i, at, :] = r[:, i * hid + fw : (i + 1) * hid]
        r = dot(hidden[...], x_cot, ((0,), (0,))).astype(BF16)
        dd[:, at] = r[:fw]
        dd_send[:, at] = r[fw:]


def expert_weight_grads(chip, blocks, gu_grad, hidden, d):
    fw = blocks[0].shape[3]
    out = (whole((2, d, fw), BF16),) * 2 + (whole((fw, d), BF16),) * 2
    return call(weight_body, out, chip, *blocks, gu_grad, hidden, scalars=1, loose=(7, 8))


def add_body(parts, out, *, half):
    n_y, n_h, rows, _ = parts.shape
    j, r = iota((out.shape[0], rows), 0), iota((out.shape[0], rows), 1)
    slot = j & 7
    source = (j >> 4) * half + slot
    total = 0.0
    for h in range(n_h):
        s = parts[0, h].astype(F32)
        for y in range(1, n_y):
            s = s + parts[y, h].astype(F32)
        hit = (source == r) & (slot < half) & (((j >> 3) & 1) == h)
        total = total + dot(jnp.where(hit, 1.0, 0.0).astype(BF16), s.astype(BF16), ((1,), (0,)))
    out[...] = total.astype(BF16)


def add_parts(parts, blocks, half):
    out = (whole((blocks * 16, parts.shape[3]), BF16),)
    return call(functools.partial(add_body, half=half), out, parts, kept=(0,))


def later(v, step, fill):
    return jnp.concatenate([v[step:], jnp.full((step, v.shape[1]), fill, v.dtype)], axis=0)


def in_three(v):
    hi = v.astype(BF16)
    mid = (v - hi.astype(F32)).astype(BF16)
    lo = (v - hi.astype(F32) - mid.astype(F32)).astype(BF16)
    return [p.astype(F32) for p in (hi, mid, lo)]


def chain_body(mix, out_proj, rec_state, decay, local, through, last):
    n_sp, width = last.shape[0], last.shape[2]
    keep = mix.shape[1] // n_sp
    proj = dot(mix[...], rec_state[...], ((0,), (0,))).astype(BF16)
    for k in range(n_sp):
        last[k, :keep, :] = proj[k * keep : (k + 1) * keep, :]
    grad = dot(mix[...], out_proj[...], ((1,), (1,)))
    mult = later(decay[...], 1, 1.0)
    step = 1
    while step < grad.shape[0]:
        grad = grad + mult * later(grad, step, 0.0)
        mult = mult * later(mult, step, 1.0)
        step *= 2
    local[...] = grad
    through[...] = mult
    first = decay[0:1, :]
    row = iota((last.shape[1] - keep, width), 0)
    chain = jnp.zeros(row.shape, F32)
    for i, piece in enumerate(in_three(first * mult[0:1, :]) + in_three(first * grad[0:1, :])):
        chain = jnp.where(row == i, piece, chain)
    chain = chain.astype(BF16)
    for k in range(n_sp):
        last[k, keep:, :] = chain


def chain_within(mix, out_proj, rec_state, decay, n_sp):
    tokens, width = decay.shape
    last = whole((n_sp, mix.shape[1] // n_sp + 8, width), BF16)
    out = (whole((tokens, width), F32),) * 2 + (last,)
    return call(chain_body, out, mix, out_proj, rec_state, decay, kept=(0, 1, 2))


def finish_body(here, last, local, through, value_by, input_by, rate_by, proj, value, inp, rate):
    n_sp = last.shape[0]
    keep = proj.shape[0]
    incoming = jnp.zeros((1, last.shape[2]), F32)
    for k in reversed(range(n_sp)):
        c = last[k, keep:, :].astype(F32)
        mult = (c[2:3] + c[1:2]) + c[0:1]
        add = (c[5:6] + c[4:5]) + c[3:4]
        incoming = jnp.where(k > here[0], add + mult * incoming, incoming)
    carried = local[...] + through[...] * incoming
    value[...] = (carried * value_by[...]).astype(BF16)
    inp[...] = (carried * input_by[...]).astype(BF16)
    rate[...] = (carried * rate_by[...]).astype(BF16)
    total = last[0, :keep, :].astype(F32)
    for k in range(1, n_sp):
        total = total + last[k, :keep, :].astype(F32)
    proj[...] = total


def finish(here, last, local, through, value_by, input_by, rate_by):
    grid = whole(local.shape, BF16)
    out = (whole((last.shape[1] - 8, last.shape[2]), F32), grid, grid, grid)
    return call(finish_body, out, here, last, local, through, value_by, input_by, rate_by, scalars=1)


def per_device(
    ffn_input,
    out_grad,
    routes,
    route_weight,
    gate_w,
    up_w,
    down_w,
    out_proj,
    rec_value,
    rate_pre,
    input_pre,
    prev_state,
    decay_param,
):
    n_sp, n_y = lax.axis_size(SP), lax.axis_size("y")
    tok, count = routes.shape
    half = 5 * count * tok // (8 * n_sp)
    fw = ffn_input.shape[1]
    d = gate_w.shape[1]
    chip = lax.axis_index("y").reshape(1).astype(jnp.int32)
    core = lax.axis_index("c").reshape(1).astype(jnp.int32)

    def over_y(v, step):
        return lax.ppermute(v, "y", [(i, (i + step) % n_y) for i in range(n_y)])

    def over_cores(v):
        return lax.ppermute(v, "c", [(0, 1), (1, 0)])

    own = jnp.stack([ffn_input, out_grad])
    far = over_y(own, n_y // 2)
    mine = jnp.stack([own, far])
    peer = over_cores(mine)
    pick, choose, scale = route_slots(core, routes.T, route_weight.T, n_sp, half)
    send = fill_slots(core, choose, scale, mine, peer)

    recv = lax.all_to_all(send.reshape(n_sp, -1, fw), SP, 0, 0, tiled=True).reshape(send.shape)
    both, near = sort_pieces(recv)

    late_gate, late_up, late_down = gate_w, up_w, down_w
    wgu = jnp.concatenate([late_gate, late_up], axis=0)
    wgu_peer = over_cores(wgu)
    wd_peer = over_cores(late_down[0])
    first = (both, over_y(both, 1), over_y(both, -1))
    blocks = (*first, over_y(near, 2), over_y(near, -2), near)

    gu_grad, hidden, part = expert_rows_grad(
        chip, blocks, wgu_peer, late_gate[0], late_up[0], late_down[0], wd_peer, n_y
    )
    rate_gate = jax.nn.sigmoid(rate_pre.astype(F32))
    input_gate = jax.nn.sigmoid(input_pre.astype(F32))
    decay_speed = jax.nn.softplus(-decay_param)[None, :]
    log_decay = -decay_scale * rate_gate * decay_speed
    decay = jnp.exp(log_decay)
    scale_in = jnp.sqrt(-jnp.expm1(2.0 * log_decay))
    signal = rec_value.astype(F32)
    before_state = prev_state.astype(F32)
    rec_state = (decay * before_state + scale_in * input_gate * signal).astype(BF16)
    value_by = scale_in * input_gate
    input_by = value_by * signal * (1.0 - input_gate)
    decay_part = decay * before_state - input_gate * signal * decay * decay / scale_in
    rate_by = decay_part * (-decay_scale * decay_speed) * rate_gate * (1.0 - rate_gate)
    here = lax.axis_index(SP).reshape(1).astype(jnp.int32)
    part, here = lax.optimization_barrier((part, here))
    arrived = lax.all_to_all(part.reshape(2 * n_y, *part.shape[2:]), TP, 0, 0, tiled=True)
    back = add_parts(arrived.reshape(part.shape), n_sp, half)
    returned = lax.all_to_all(back.reshape(n_sp, 16, fw), SP, 0, 0, tiled=True).reshape(back.shape)
    dgu, dgu_send, dd, dd_send = expert_weight_grads(chip, blocks, gu_grad, hidden, d)
    dgu_peer = over_cores(dgu_send)
    dd_peer = over_cores(dd_send)
    d_gate, d_up = [(dgu[i].astype(F32) + dgu_peer[i].astype(F32)).astype(BF16)[None] for i in range(2)]
    d_down = (dd.astype(F32) + dd_peer.astype(F32)).astype(BF16)[None]
    own_grad = (dot(pick, returned, ((0,), (0,))) + out_grad.astype(F32)).astype(BF16)
    mix_grad = lax.all_gather(own_grad, TP, axis=1, tiled=True)

    local, through, last = chain_within(mix_grad, out_proj, rec_state, decay, n_sp)
    last = lax.all_to_all(last, SP, 0, 0, tiled=True)
    out_proj_grad, rec_value_grad, input_pre_grad, rate_pre_grad = finish(
        here, last, local, through, value_by, input_by, rate_by
    )
    return (
        d_gate,
        d_up,
        d_down,
        out_proj_grad,
        rec_value_grad,
        rate_pre_grad,
        input_pre_grad,
    )


def solution(mesh):
    finer = Mesh(mesh.devices.reshape(8, 4, 8, 2), ("z", "x", "y", "c"))
    grid = P(SP, TP)
    return jax.shard_map(
        per_device,
        mesh=finer,
        in_specs=(
            grid,
            grid,
            P(SP, None),
            P(SP, None),
            P(SP, None, TP),
            P(SP, None, TP),
            P(SP, TP, None),
            P(TP, None),
            grid,
            grid,
            grid,
            grid,
            P(TP),
        ),
        out_specs=(P(SP, None, TP), P(SP, None, TP), P(SP, TP, None), grid, grid, grid, grid),
        check_vma=False,
    )
```
